256 devices in a mesh: tp: 16 (over y, x), dp: 16 (over z, core).
Axes of the slice: x: 4, y: 4, z: 8, core: 2. Of those that a mesh axis runs over, the one named last changes fastest.
Arguments:
- tokens: bfloat16 [256, 4096], P(None, 'dp'), may hold values from -15 to 15, as said below
- norm_gain: float32 [2, 4096], P(None, 'dp'), may hold values from 0.1 to 1.9
- w_query: bfloat16 [2, 4096, 2048], P(None, 'dp', 'tp'), may hold values from -0.09375 to 0.09375
- w_forget: bfloat16 [2, 4096, 2048], P(None, 'dp', 'tp'), may hold values from -0.09375 to 0.09375
- w_value: bfloat16 [2, 4096, 2048], P(None, 'dp', 'tp'), may hold values from -0.09375 to 0.09375
- w_gate: bfloat16 [2, 4096, 2048], P(None, 'dp', 'tp'), may hold values from -0.09375 to 0.09375
- floor_rate: float32 [2, 2048], P(None, 'tp'), may hold values from 0 to 0.9
- head_gain: float32 [2, 128], replicated, may hold values from 0.1 to 1.9
- w_output: bfloat16 [2, 2048, 4096], P(None, 'tp', 'dp'), may hold values from -0.3 to 0.3
- state: float32 [2, 256, 16, 128, 128], P(None, 'dp', 'tp'), may hold values from -4 to 4
Outputs:
- mixed: bfloat16 [256, 4096], P(None, 'dp')
- new_state: float32 [2, 256, 16, 128, 128], P(None, 'dp', 'tp')
The draws below stay inside these ranges and needn't reach their ends.
Inputs may be any that keep to these rules, and one draw needn't show every extreme that they name: `tokens`: activations whose feature blocks have different scales.
All inputs are finite; a program needn't handle non-finite values.
Results may differ from the reference program's by a relative error of at most 0.035.
Values may be sent and summed in bfloat16 or wider, within the bound.
A program may use at most 64 MiB of HBM per device.

```python
import jax
import jax.numpy as jnp
from jax import lax

D = 4096
H = 16
DK = 128
DV = 128
BATCH = 256
N_DP = 16


def draw_tokens(key, part):
    first, second, third = jax.random.split(key, 3)
    group_scales = jnp.exp(jax.random.uniform(second, (32,), jnp.float32, jnp.log(0.25), jnp.log(2.5)))
    column_scales = jnp.repeat(group_scales, D // 32)
    base = jnp.clip(jax.random.normal(first, (BATCH, D), jnp.float32), -5.9, 5.9)
    return (base * column_scales[None, :]).astype(jnp.bfloat16)


def draw_w_output(key, part):
    rows = H * DV
    keys = jax.random.split(jax.random.fold_in(key, 71), 5)
    even_signs = 2.0 * jax.random.randint(keys[0], (2, rows, 1), 0, 2).astype(jnp.float32) - 1.0
    odd_signs = 2.0 * jax.random.randint(keys[1], (2, rows, 1), 0, 2).astype(jnp.float32) - 1.0
    column_signs = 2.0 * jax.random.randint(keys[2], (2, 1, D), 0, 2).astype(jnp.float32) - 1.0
    block_parity = (jnp.arange(D) // (D // N_DP) % 2)[None, None, :]
    pattern = jnp.where(block_parity == 0, even_signs, odd_signs)
    sigma = 1.5 / jnp.sqrt(jnp.float32(rows))
    magnitude = jax.random.uniform(keys[3], (2, 1, D), jnp.float32, 0.02, 0.06)
    noise = jnp.clip(jax.random.normal(keys[4], (2, rows, D), jnp.float32), -5.0, 5.0) * sigma
    total = jnp.clip(pattern * column_signs * magnitude + noise, -0.298, 0.298)
    return total.astype(jnp.bfloat16)


def block_scale(own_key, extent, cuts, low, largest):
    gain = 1.0
    for dim, parts in cuts:
        heights = jax.random.uniform(jax.random.fold_in(jax.random.fold_in(own_key, 6), dim), (parts,), jnp.float32, low / len(cuts), largest / len(cuts))
        gain = gain * jnp.repeat(jnp.exp(heights), extent[dim] // parts).reshape((-1,) + (1,) * (len(extent) - 1 - dim))
    return gain


def normal_values(own_key, extent, spread, limit, cuts=(), held_as=jnp.bfloat16):
    level = block_scale(own_key, extent, cuts, -0.22, 0.18) if cuts else 1.0
    array = jax.random.normal(own_key, extent, jnp.float32) * spread * level
    return jnp.minimum(jnp.maximum(array, -limit), limit).astype(held_as)


def setup_inputs(seed: int = 0) -> dict:
    streams_of = jax.random.split(jax.random.key(seed), 11)
    return {
        "tokens": draw_tokens(jax.random.fold_in(streams_of[10], 71), 0),
        "norm_gain": jnp.clip(1.0 + 0.18 * jax.random.normal(streams_of[1], (2, D), jnp.float32), 0.1, 1.9),
        "w_query": normal_values(streams_of[2], (2, D, H * DK), D ** -0.5, 0.09375, ((1, 16), (2, 16))),
        "w_forget": normal_values(streams_of[3], (2, D, H * DK), D ** -0.5, 0.09375, ((1, 16), (2, 16))),
        "w_value": normal_values(streams_of[4], (2, D, H * DV), D ** -0.5, 0.09375, ((1, 16), (2, 16))),
        "w_gate": normal_values(streams_of[5], (2, D, H * DV), D ** -0.5, 0.09375, ((1, 16), (2, 16))),
        "floor_rate": jnp.clip(0.9 * jax.random.uniform(streams_of[6], (2, H * DK), jnp.float32) ** block_scale(streams_of[6], (2, H * DK), ((1, 16),), -0.2, 0.2), 0.0, 0.9),
        "head_gain": jnp.clip(1.0 + 0.18 * jax.random.normal(streams_of[7], (2, DV), jnp.float32), 0.1, 1.9),
        "w_output": draw_w_output(jax.random.fold_in(streams_of[10], 71), 0),
        "state": normal_values(streams_of[9], (2, BATCH, H, DK, DV), 0.5, 4.0, ((1, 16), (2, 16)), jnp.float32),
    }


EPS = 1e-06

def mixer_layer(tokens, norm_gain, w_query, w_forget, w_value, w_gate, floor_rate, head_gain, w_output, old_state):
    tok = tokens.astype(jnp.float32)
    row_scale = lax.rsqrt(lax.optimization_barrier(jnp.mean(tok * tok, axis=-1, keepdims=True)) + EPS)
    normed = (tok * norm_gain).astype(jnp.bfloat16)
    blocks = normed.reshape(BATCH, N_DP, D // N_DP).astype(jnp.float32)

    def project(weight):
        pieces = weight.reshape(N_DP, D // N_DP, weight.shape[1]).astype(jnp.float32)
        partial_terms = jnp.einsum('bnd,ndc->nbc', blocks, pieces)
        rounded = lax.optimization_barrier(partial_terms.astype(jnp.bfloat16))
        total = lax.optimization_barrier(jnp.sum(rounded.astype(jnp.float32), axis=0))
        stored = lax.optimization_barrier((row_scale * total).astype(jnp.bfloat16))
        return stored.astype(jnp.float32).reshape(BATCH, H, -1)
    query = jax.nn.silu(project(w_query)) * DK ** (-0.5)
    forget_pre = project(w_forget)
    value = project(w_value)
    gate_pre = project(w_gate)
    floor_heads = floor_rate.reshape(H, DK)
    forget = floor_heads + (1.0 - floor_heads) * jax.nn.sigmoid(forget_pre)
    key_in = (1.0 - floor_heads) * jax.nn.sigmoid(-forget_pre)
    updated = old_state * forget[..., None] + key_in[..., None] * value[:, :, None, :]
    read = jnp.einsum('bhk,bhkv->bhv', query, updated, precision=lax.Precision.HIGHEST)
    read = read * lax.rsqrt(lax.optimization_barrier(jnp.mean(read * read, axis=-1, keepdims=True)) + EPS) * head_gain
    gated = (read * jax.nn.silu(gate_pre)).reshape(BATCH, H * DV).astype(jnp.bfloat16)
    update = jnp.dot(gated, w_output, preferred_element_type=jnp.float32)
    return ((tok + update).astype(jnp.bfloat16), updated)

def reference(tokens, norm_gain, w_query, w_forget, w_value, w_gate, floor_rate, head_gain, w_output, state):
    current = tokens
    states = []
    for layer_index in range(2):
        current, updated = mixer_layer(current, norm_gain[layer_index], w_query[layer_index], w_forget[layer_index], w_value[layer_index], w_gate[layer_index], floor_rate[layer_index], head_gain[layer_index], w_output[layer_index], state[layer_index])
        states.append(updated)
    return (current, jnp.stack(states, axis=0))
```

```python
import functools

import jax
import jax.numpy as jnp
from jax import lax
from jax.experimental import pallas as pl
from jax.experimental.pallas import tpu as pltpu
from jax.sharding import PartitionSpec as P

D = 4096
DK = 128
EPS = 1e-06
MESH = pl.DeviceIdType.MESH
F32 = jnp.float32
BF16 = jnp.bfloat16

Z_ORDER = (0, 1, 7, 2, 6, 3, 5, 4)
C_GROUPS = ((0, 6), (6, 10), (10, 16))
E_GROUPS = (0, 2, 3, 1)


def gray(v):
    return v + v // 2 - 2 * (v // 3)


def tp_slot(dy, dx):
    return (dx % 2) * 8 + (dx // 2) * 4 + gray(dy)


def z_slot(dz, rel):
    return 2 * Z_ORDER.index(dz) + rel


def z_slot_traced(dz, rel):
    pos = jnp.where(dz <= 4, 2 * dz - jnp.minimum(dz, 1), 16 - 2 * dz)
    return 2 * pos + rel


def kernel(
    tok_in,
    gain_in,
    wq_in,
    wf_in,
    wv_in,
    wg_in,
    floor_in,
    hgain_in,
    wout_in,
    state_in,
    mixed_out,
    state_out,
    cur,
    gain,
    w,
    floor,
    hgain,
    wout,
    old,
    part,
    pair_in,
    pair,
    sums_in,
    sq,
    sq_pair_in,
    sq_pair,
    sq_in,
    gat,
    upd,
    upd_in,
    final,
    load_sem,
    tok_sem,
    a1_send,
    a1_recv,
    s1_send,
    s1_recv,
    a2_send,
    a2_recv,
    s2_send,
    s2_recv,
    c_send,
    c_recv,
    d_send,
    d_recv,
    e_send,
    e_recv,
):
    h = lax.axis_index("tp")
    d = lax.axis_index("dp")
    y, x = h // 4, h % 4
    z, core = d // 2, d % 2
    e = (x + core) % 2
    partner = {"dp": 2 * z + 1 - core}

    barrier = pltpu.get_barrier_semaphore()
    for k in range(1, 16):
        pl.semaphore_signal(barrier, inc=1, device_id={"tp": (h + k) % 16}, device_id_type=MESH)
        pl.semaphore_signal(barrier, inc=1, device_id={"dp": (d + k) % 16}, device_id_type=MESH)

    toks = []
    for dy in range(4):
        for dx in range(4):
            rows = ((y + dy) % 4) * 4 + (x + dx) % 4
            copy = pltpu.make_async_copy(
                tok_in.at[pl.ds(rows * 16, 16), :], cur.at[0, tp_slot(dy, dx)], tok_sem
            )
            copy.start()
    tok_all = pltpu.make_async_copy(cur.at[0], cur.at[0], tok_sem)

    loads = {}

    def load(name, src, dst):
        loads[name] = pltpu.make_async_copy(src, dst, load_sem.at[len(loads)])
        loads[name].start()

    weights = (wq_in, wf_in, wv_in, wg_in)
    load("gain", gain_in, gain)
    for n in range(4):
        load(("w", 0, n), weights[n].at[0], w.at[0, :, pl.ds(128 * n, 128)])
    load("floor", floor_in, floor)
    load("hgain", hgain_in, hgain)
    load(("state", 0), state_in.at[0, :, 0], old.at[0])
    load(("wout", 0), wout_in.at[0], wout.at[0])
    for n in range(4):
        load(("w", 1, n), weights[n].at[1], w.at[1, :, pl.ds(128 * n, 128)])
    load(("state", 1), state_in.at[1, :, 0], old.at[1])
    load(("wout", 1), wout_in.at[1], wout.at[1])

    own = pl.multiple_of(8 * e, 8)
    other = pl.multiple_of(8 - 8 * e, 8)
    self_dy = ((2 * z + core) // 4 - y + 4) % 4
    self_dx = ((2 * z + core) % 4 - x + 4) % 4
    self_slot = (self_dx // 2) * 4 + gray(self_dy)
    up_dz = (h // 2 - z + 8) % 8
    up_rel = (h % 2 + core) % 2
    up_slot = z_slot_traced(up_dz, up_rel)

    def remote(src, dst, send, recv, device):
        return pltpu.make_async_remote_copy(
            src_ref=src,
            dst_ref=dst,
            send_sem=send,
            recv_sem=recv,
            device_id=device,
            device_id_type=MESH,
        )

    def wait_bytes(ref, sem):
        pltpu.make_async_copy(ref, ref, sem).wait()

    def project(l, first, count):
        rows = cur[l, pl.ds(first, count)].astype(F32).reshape(16 * count, 256)
        normed = (rows * gain[l : l + 1, :]).astype(BF16)
        product = jnp.dot(normed, w[l], preferred_element_type=F32)
        part[l, pl.ds(first, count)] = product.astype(BF16).reshape(count, 16, 512)

    def squares(l):
        ones = jnp.ones((8, 256), BF16)
        for c in range(2):
            rows = cur[l, 8 * c : 8 * c + 8].astype(F32).reshape(128, 256)
            square = rows * rows
            high = square.astype(BF16)
            low = (square - high.astype(F32)).astype(BF16)
            dims = (((1,), (1,)), ((), ()))
            total = lax.dot_general(ones, high, dims, preferred_element_type=F32)
            total += lax.dot_general(ones, low, dims, preferred_element_type=F32)
            sq[l, c] = total[:1]

    def send_pair(l, half):
        remote(
            part.at[l, pl.ds(other + 4 * half, 4)],
            pair_in.at[l, pl.ds(4 * half, 4)],
            a1_send.at[l, half],
            a1_recv.at[l, half],
            partner,
        ).start()

    def send_squares(l):
        remote(sq.at[l, 1 - e], sq_pair_in.at[l], s1_send.at[l], s1_recv.at[l], partner).start()

    for l in range(2):
        if l == 0:
            tok_all.wait()
            loads["gain"].wait()
            for n in range(4):
                loads["w", 0, n].wait()
            project(0, other, 8)
            squares(0)
            pl.semaphore_wait(barrier, 30)
            send_squares(0)
            send_pair(0, 0)
            send_pair(0, 1)
            project(0, own, 8)
        else:
            for n in range(4):
                loads["w", 1, n].wait()
            for group in E_GROUPS:
                arrived = 3 if group == 0 else 4
                wait_bytes(cur.at[1, pl.ds(0, arrived)], e_recv.at[0, group])
                project(1, 4 * group, 4)

                @pl.when(e != group // 2)
                def _():
                    send_pair(1, group % 2)

            squares(1)
            send_squares(1)

        wait_bytes(sq_pair_in.at[l], s1_recv.at[l])
        sq_pair[l] = sq[l, e] + sq_pair_in[l]
        for k in range(1, 8):
            remote(
                sq_pair.at[l],
                sq_in.at[l, 8 - k],
                s2_send.at[l],
                s2_recv.at[l],
                {"dp": (d + 2 * k) % 16},
            ).start()
        for half in range(2):
            wait_bytes(pair_in.at[l, pl.ds(0, 4)], a1_recv.at[l, half])
            mine = part[l, pl.ds(own + 4 * half, 4)].astype(F32)
            theirs = pair_in[l, 4 * half : 4 * half + 4].astype(F32)
            pair[l, 4 * half : 4 * half + 4] = (mine + theirs).astype(BF16)
            for i in range(4):
                block = ((y + gray(i)) % 4) * 4 + (x + 2 * half + e) % 4
                to_z = block // 2

                @pl.when(to_z != z)
                def _():
                    remote(
                        pair.at[l, 4 * half + i],
                        sums_in.at[l, (z - to_z + 8) % 8],
                        a2_send.at[l],
                        a2_recv.at[l],
                        {"dp": 2 * to_z + core},
                    ).start()

        wait_bytes(sq_in.at[l, pl.ds(0, 7)], s2_recv.at[l])
        row = sq_pair[l]
        for k in range(1, 8):
            row = row + sq_in[l, k]
        lanes = lax.broadcasted_iota(jnp.int32, (16, 128), 1)
        rows = lax.broadcasted_iota(jnp.int32, (16, 128), 0)
        picked = jnp.where(lanes == rows + 16 * self_slot, jnp.broadcast_to(row, (16, 128)), 0.0)
        row_scale = lax.rsqrt(jnp.sum(picked, axis=1, keepdims=True) / D + EPS)
        if l == 0:
            loads["floor"].wait()
            loads["hgain"].wait()
        loads["state", l].wait()
        wait_bytes(sums_in.at[l, pl.ds(0, 7)], a2_recv.at[l])
        total = pair[l, self_slot].astype(F32)
        for k in range(1, 8):
            total = total + sums_in[l, k].astype(F32)
        stored = (row_scale * total).astype(BF16).astype(F32)
        query_pre, forget_pre = stored[:, :128], stored[:, 128:256]
        value, gate_pre = stored[:, 256:384], stored[:, 384:]
        query = jax.nn.silu(query_pre) * DK ** (-0.5)
        low = floor[l : l + 1, :]
        forget = low + (1.0 - low) * jax.nn.sigmoid(forget_pre)
        key_in = (1.0 - low) * jax.nn.sigmoid(-forget_pre)
        scaled = (query * forget).T
        reads = []
        for b in range(16):
            reads.append(jnp.sum(old[l, b] * scaled[:, b : b + 1], axis=0, keepdims=True))
        read = jnp.concatenate(reads, axis=0)
        read = read + jnp.sum(query * key_in, axis=1, keepdims=True) * value
        read = read * lax.rsqrt(jnp.mean(read * read, axis=1, keepdims=True) + EPS)
        gated = read * hgain[l : l + 1, :] * jax.nn.silu(gate_pre)
        gat[l, 0] = gated.astype(BF16)

        for dz in reversed(Z_ORDER):
            for rel in (1, 0):
                if dz == 0 and rel == 0:
                    continue
                slot = z_slot((8 - dz) % 8, rel)
                to_core = core if rel == 0 else 1 - core
                group = [slot >= first and slot < last for first, last in C_GROUPS].index(True)
                remote(
                    gat.at[l, 0],
                    gat.at[l, slot],
                    c_send.at[l],
                    c_recv.at[l, group],
                    {"dp": 2 * ((z + dz) % 8) + to_core},
                ).start()

        forget_t, key_t = forget.T, key_in.T
        for b in range(16):
            kept = old[l, b] * forget_t[:, b : b + 1]
            state_out[l, b, 0] = kept + key_t[:, b : b + 1] * value[b : b + 1, :]

        loads["wout", l].wait()
        for group, (first, last) in enumerate(C_GROUPS):
            arrived = last - first - (1 if group == 0 else 0)
            wait_bytes(gat.at[l, pl.ds(0, arrived)], c_recv.at[l, group])
            rows = gat[l, first:last].reshape(16 * (last - first), 128)
            product = jnp.dot(rows, wout[l], preferred_element_type=F32)
            upd[l, first:last] = product.astype(BF16).reshape(last - first, 16, 256)
            for slot in range(first, last):
                dz, rel = Z_ORDER[slot // 2], slot % 2
                to_core = core if rel == 0 else 1 - core
                owner = 2 * ((z + dz) % 8) + to_core
                dy = (y - owner // 4 + 4) % 4
                dx = (x - owner % 4 + 4) % 4

                @pl.when(owner != h)
                def _():
                    remote(
                        upd.at[l, slot],
                        upd_in.at[l, tp_slot(dy, dx)],
                        d_send.at[l],
                        d_recv.at[l],
                        {"tp": owner},
                    ).start()

        wait_bytes(upd_in.at[l, pl.ds(0, 15)], d_recv.at[l])
        share = upd[l, up_slot].astype(F32)
        for s in range(1, 16):
            share = share + upd_in[l, s].astype(F32)
        fresh = (cur[l, 0].astype(F32) + share).astype(BF16)

        if l == 0:
            cur[1, 0] = fresh
        else:
            final[h] = fresh
        offsets = [(dy, dx) for dy in range(4) for dx in range(4) if dy or dx]
        near = (0, 1, 2, 1)
        offsets.sort(key=lambda o: -near[o[0]] - near[o[1]])
        for dy, dx in offsets:
            to = ((y + dy) % 4) * 4 + (x + dx) % 4
            slot = tp_slot((4 - dy) % 4, (4 - dx) % 4)
            if l == 0:
                src, dst, recv = cur.at[1, 0], cur.at[1, slot], e_recv.at[0, slot // 4]
            else:
                src, dst, recv = final.at[h], final.at[h], e_recv.at[1, 0]
            remote(src, dst, e_send.at[l], recv, {"tp": to}).start()

    for l in range(2):
        wait_bytes(sq_pair_in.at[l], s1_send.at[l])
        wait_bytes(sq_in.at[l, pl.ds(0, 7)], s2_send.at[l])
        for half in range(2):
            wait_bytes(pair_in.at[l, pl.ds(0, 4)], a1_send.at[l, half])
        wait_bytes(sums_in.at[l, pl.ds(0, 7)], a2_send.at[l])
        wait_bytes(gat.at[l, pl.ds(0, 15)], c_send.at[l])
        wait_bytes(upd_in.at[l, pl.ds(0, 15)], d_send.at[l])
        wait_bytes(cur.at[0, pl.ds(0, 15)], e_send.at[l])
    wait_bytes(final.at[pl.ds(0, 15)], e_recv.at[1, 0])
    mixed_out[...] = final[...].reshape(256, 256)


def per_device(*args):
    any_spec = pl.BlockSpec(memory_space=pl.ANY)
    vmem_spec = pl.BlockSpec(memory_space=pltpu.VMEM)
    dma = pltpu.SemaphoreType.DMA
    return pl.pallas_call(
        kernel,
        out_shape=(
            jax.ShapeDtypeStruct((256, 256), BF16),
            jax.ShapeDtypeStruct((2, 16, 1, 128, 128), F32),
        ),
        in_specs=[any_spec] * 10,
        out_specs=(vmem_spec, vmem_spec),
        scratch_shapes=[
            pltpu.VMEM((2, 16, 16, 256), BF16),
            pltpu.VMEM((2, 256), F32),
            pltpu.VMEM((2, 256, 512), BF16),
            pltpu.VMEM((2, 128), F32),
            pltpu.VMEM((2, 128), F32),
            pltpu.VMEM((2, 128, 256), BF16),
            pltpu.VMEM((2, 16, 128, 128), F32),
            pltpu.VMEM((2, 16, 16, 512), BF16),
            pltpu.VMEM((2, 8, 16, 512), BF16),
            pltpu.VMEM((2, 8, 16, 512), BF16),
            pltpu.VMEM((2, 8, 16, 512), BF16),
            pltpu.VMEM((2, 2, 1, 128), F32),
            pltpu.VMEM((2, 1, 128), F32),
            pltpu.VMEM((2, 1, 128), F32),
            pltpu.VMEM((2, 8, 1, 128), F32),
            pltpu.VMEM((2, 16, 16, 128), BF16),
            pltpu.VMEM((2, 16, 16, 256), BF16),
            pltpu.VMEM((2, 16, 16, 256), BF16),
            pltpu.VMEM((16, 16, 256), BF16),
            dma((17,)),
            dma,
            dma((2, 2)),
            dma((2, 2)),
            dma((2,)),
            dma((2,)),
            dma((2,)),
            dma((2,)),
            dma((2,)),
            dma((2,)),
            dma((2,)),
            dma((2, 3)),
            dma((2,)),
            dma((2,)),
            dma((2,)),
            dma((2, 4)),
        ],
        compiler_params=pltpu.CompilerParams(collective_id=0, has_side_effects=True),
    )(*args)


def solution(mesh):
    in_specs = (
        P(None, "dp"),
        P(None, "dp"),
        P(None, "dp", "tp"),
        P(None, "dp", "tp"),
        P(None, "dp", "tp"),
        P(None, "dp", "tp"),
        P(None, "tp"),
        P(),
        P(None, "tp", "dp"),
        P(None, "dp", "tp", None, None),
    )
    out_specs = (P(None, "dp"), P(None, "dp", "tp", None, None))
    return jax.shard_map(
        per_device, mesh=mesh, in_specs=in_specs, out_specs=out_specs, check_vma=False
    )
```

```python
import functools

import jax
import jax.numpy as jnp
from jax import lax
from jax.experimental import pallas as pl
from jax.experimental.pallas import tpu as pltpu
from jax.sharding import PartitionSpec as P

D = 4096
DK = 128
EPS = 1e-06
MESH = pl.DeviceIdType.MESH
F32 = jnp.float32
BF16 = jnp.bfloat16

Z_ORDER = (0, 1, 7, 2, 6, 3, 5, 4)
C_GROUPS = ((0, 6), (6, 10), (10, 16))
E_GROUPS = (0, 2, 3, 1)


def gray(v):
    return v + v // 2 - 2 * (v // 3)


def tp_slot(dy, dx):
    return (dx % 2) * 8 + (dx // 2) * 4 + gray(dy)


def z_slot(dz, rel):
    return 2 * Z_ORDER.index(dz) + rel


def z_slot_traced(dz, rel):
    pos = jnp.where(dz <= 4, 2 * dz - jnp.minimum(dz, 1), 16 - 2 * dz)
    return 2 * pos + rel


def kernel(
    tok_in,
    gain_in,
    wq_in,
    wf_in,
    wv_in,
    wg_in,
    floor_in,
    hgain_in,
    wout_in,
    state_in,
    mixed_out,
    state_out,
    cur,
    gain,
    w,
    floor,
    hgain,
    wout,
    old,
    part,
    pair_in,
    pair,
    sums_in,
    sq,
    sq_pair_in,
    sq_pair,
    sq_in,
    gat,
    upd,
    upd_in,
    final,
    load_sem,
    tok_sem,
    a1_send,
    a1_recv,
    s1_send,
    s1_recv,
    a2_send,
    a2_recv,
    s2_send,
    s2_recv,
    c_send,
    c_recv,
    d_send,
    d_recv,
    e_send,
    e_recv,
):
    h = lax.axis_index("tp")
    d = lax.axis_index("dp")
    y, x = h // 4, h % 4
    z, core = d // 2, d % 2
    e = (x + core) % 2
    partner = {"dp": 2 * z + 1 - core}

    toks = []
    for dy in range(4):
        for dx in range(4):
            rows = ((y + dy) % 4) * 4 + (x + dx) % 4
            copy = pltpu.make_async_copy(
                tok_in.at[pl.ds(rows * 16, 16), :], cur.at[0, tp_slot(dy, dx)], tok_sem
            )
            copy.start()
    tok_all = pltpu.make_async_copy(cur.at[0], cur.at[0], tok_sem)

    loads = {}

    def load(name, src, dst):
        loads[name] = pltpu.make_async_copy(src, dst, load_sem.at[len(loads)])
        loads[name].start()

    weights = (wq_in, wf_in, wv_in, wg_in)
    load("gain", gain_in, gain)
    for n in range(4):
        load(("w", 0, n), weights[n].at[0], w.at[0, :, pl.ds(128 * n, 128)])
    barrier = pltpu.get_barrier_semaphore()
    for k in range(1, 16):
        pl.semaphore_signal(barrier, inc=1, device_id={"tp": (h + k) % 16}, device_id_type=MESH)
        pl.semaphore_signal(barrier, inc=1, device_id={"dp": (d + k) % 16}, device_id_type=MESH)

    own = pl.multiple_of(8 * e, 8)
    other = pl.multiple_of(8 - 8 * e, 8)
    self_dy = ((2 * z + core) // 4 - y + 4) % 4
    self_dx = ((2 * z + core) % 4 - x + 4) % 4
    self_slot = (self_dx // 2) * 4 + gray(self_dy)
    up_dz = (h // 2 - z + 8) % 8
    up_rel = (h % 2 + core) % 2
    up_slot = z_slot_traced(up_dz, up_rel)

    def remote(src, dst, send, recv, device):
        return pltpu.make_async_remote_copy(
            src_ref=src,
            dst_ref=dst,
            send_sem=send,
            recv_sem=recv,
            device_id=device,
            device_id_type=MESH,
        )

    def wait_bytes(ref, sem):
        pltpu.make_async_copy(ref, ref, sem).wait()

    def project(l, first, count):
        rows = cur[l, pl.ds(first, count)].astype(F32).reshape(16 * count, 256)
        normed = (rows * gain[l : l + 1, :]).astype(BF16)
        product = jnp.dot(normed, w[l], preferred_element_type=F32)
        part[l, pl.ds(first, count)] = product.astype(BF16).reshape(count, 16, 512)

    def squares(l):
        ones = jnp.ones((8, 256), BF16)
        for c in range(2):
            rows = cur[l, 8 * c : 8 * c + 8].astype(F32).reshape(128, 256)
            square = rows * rows
            high = square.astype(BF16)
            low = (square - high.astype(F32)).astype(BF16)
            dims = (((1,), (1,)), ((), ()))
            total = lax.dot_general(ones, high, dims, preferred_element_type=F32)
            total += lax.dot_general(ones, low, dims, preferred_element_type=F32)
            sq[l, c] = total[:1]

    def send_pair(l, half):
        remote(
            part.at[l, pl.ds(other + 4 * half, 4)],
            pair_in.at[l, pl.ds(4 * half, 4)],
            a1_send.at[l, half],
            a1_recv.at[l, half],
            partner,
        ).start()

    def send_squares(l):
        remote(sq.at[l, 1 - e], sq_pair_in.at[l], s1_send.at[l], s1_recv.at[l], partner).start()

    for l in range(2):
        if l == 0:
            tok_all.wait()
            loads["gain"].wait()
            for n in range(4):
                loads["w", 0, n].wait()
            project(0, other, 8)
            load("floor", floor_in, floor)
            load("hgain", hgain_in, hgain)
            load(("state", 0), state_in.at[0, :, 0], old.at[0])
            load(("wout", 0), wout_in.at[0], wout.at[0])
            for n in range(4):
                load(("w", 1, n), weights[n].at[1], w.at[1, :, pl.ds(128 * n, 128)])
            load(("state", 1), state_in.at[1, :, 0], old.at[1])
            load(("wout", 1), wout_in.at[1], wout.at[1])
            squares(0)
            pl.semaphore_wait(barrier, 30)
            send_squares(0)
            send_pair(0, 0)
            send_pair(0, 1)
            project(0, own, 8)
        else:
            for n in range(4):
                loads["w", 1, n].wait()
            for group in E_GROUPS:
                arrived = 3 if group == 0 else 4
                wait_bytes(cur.at[1, pl.ds(0, arrived)], e_recv.at[0, group])
                project(1, 4 * group, 4)

                @pl.when(e != group // 2)
                def _():
                    send_pair(1, group % 2)

            squares(1)
            send_squares(1)

        wait_bytes(sq_pair_in.at[l], s1_recv.at[l])
        sq_pair[l] = sq[l, e] + sq_pair_in[l]
        for k in range(1, 8):
            remote(
                sq_pair.at[l],
                sq_in.at[l, 8 - k],
                s2_send.at[l],
                s2_recv.at[l],
                {"dp": (d + 2 * k) % 16},
            ).start()
        for half in range(2):
            wait_bytes(pair_in.at[l, pl.ds(0, 4)], a1_recv.at[l, half])
            mine = part[l, pl.ds(own + 4 * half, 4)].astype(F32)
            theirs = pair_in[l, 4 * half : 4 * half + 4].astype(F32)
            pair[l, 4 * half : 4 * half + 4] = (mine + theirs).astype(BF16)
            for i in range(4):
                block = ((y + gray(i)) % 4) * 4 + (x + 2 * half + e) % 4
                to_z = block // 2

                @pl.when(to_z != z)
                def _():
                    remote(
                        pair.at[l, 4 * half + i],
                        sums_in.at[l, (z - to_z + 8) % 8],
                        a2_send.at[l],
                        a2_recv.at[l],
                        {"dp": 2 * to_z + core},
                    ).start()

        wait_bytes(sq_in.at[l, pl.ds(0, 7)], s2_recv.at[l])
        row = sq_pair[l]
        for k in range(1, 8):
            row = row + sq_in[l, k]
        lanes = lax.broadcasted_iota(jnp.int32, (16, 128), 1)
        rows = lax.broadcasted_iota(jnp.int32, (16, 128), 0)
        picked = jnp.where(lanes == rows + 16 * self_slot, jnp.broadcast_to(row, (16, 128)), 0.0)
        row_scale = lax.rsqrt(jnp.sum(picked, axis=1, keepdims=True) / D + EPS)
        if l == 0:
            loads["floor"].wait()
            loads["hgain"].wait()
        loads["state", l].wait()
        wait_bytes(sums_in.at[l, pl.ds(0, 7)], a2_recv.at[l])
        total = pair[l, self_slot].astype(F32)
        for k in range(1, 8):
            total = total + sums_in[l, k].astype(F32)
        stored = (row_scale * total).astype(BF16).astype(F32)
        query_pre, forget_pre = stored[:, :128], stored[:, 128:256]
        value, gate_pre = stored[:, 256:384], stored[:, 384:]
        query = jax.nn.silu(query_pre) * DK ** (-0.5)
        low = floor[l : l + 1, :]
        forget = low + (1.0 - low) * jax.nn.sigmoid(forget_pre)
        key_in = (1.0 - low) * jax.nn.sigmoid(-forget_pre)
        scaled = (query * forget).T
        reads = []
        for b in range(16):
            reads.append(jnp.sum(old[l, b] * scaled[:, b : b + 1], axis=0, keepdims=True))
        read = jnp.concatenate(reads, axis=0)
        read = read + jnp.sum(query * key_in, axis=1, keepdims=True) * value
        read = read * lax.rsqrt(jnp.mean(read * read, axis=1, keepdims=True) + EPS)
        gated = read * hgain[l : l + 1, :] * jax.nn.silu(gate_pre)
        gat[l, 0] = gated.astype(BF16)

        for dz in reversed(Z_ORDER):
            for rel in (1, 0):
                if dz == 0 and rel == 0:
                    continue
                slot = z_slot((8 - dz) % 8, rel)
                to_core = core if rel == 0 else 1 - core
                group = [slot >= first and slot < last for first, last in C_GROUPS].index(True)
                remote(
                    gat.at[l, 0],
                    gat.at[l, slot],
                    c_send.at[l],
                    c_recv.at[l, group],
                    {"dp": 2 * ((z + dz) % 8) + to_core},
                ).start()

        forget_t, key_t = forget.T, key_in.T
        for b in range(16):
            kept = old[l, b] * forget_t[:, b : b + 1]
            state_out[l, b, 0] = kept + key_t[:, b : b + 1] * value[b : b + 1, :]

        loads["wout", l].wait()
        for group, (first, last) in enumerate(C_GROUPS):
            arrived = last - first - (1 if group == 0 else 0)
            wait_bytes(gat.at[l, pl.ds(0, arrived)], c_recv.at[l, group])
            rows = gat[l, first:last].reshape(16 * (last - first), 128)
            product = jnp.dot(rows, wout[l], preferred_element_type=F32)
            upd[l, first:last] = product.astype(BF16).reshape(last - first, 16, 256)
            for slot in range(first, last):
                dz, rel = Z_ORDER[slot // 2], slot % 2
                to_core = core if rel == 0 else 1 - core
                owner = 2 * ((z + dz) % 8) + to_core
                dy = (y - owner // 4 + 4) % 4
                dx = (x - owner % 4 + 4) % 4

                @pl.when(owner != h)
                def _():
                    remote(
                        upd.at[l, slot],
                        upd_in.at[l, tp_slot(dy, dx)],
                        d_send.at[l],
                        d_recv.at[l],
                        {"tp": owner},
                    ).start()

        wait_bytes(upd_in.at[l, pl.ds(0, 15)], d_recv.at[l])
        share = upd[l, up_slot].astype(F32)
        for s in range(1, 16):
            share = share + upd_in[l, s].astype(F32)
        fresh = (cur[l, 0].astype(F32) + share).astype(BF16)

        if l == 0:
            cur[1, 0] = fresh
        else:
            final[h] = fresh
        offsets = [(dy, dx) for dy in range(4) for dx in range(4) if dy or dx]
        near = (0, 1, 2, 1)
        offsets.sort(key=lambda o: -near[o[0]] - near[o[1]])
        for dy, dx in offsets:
            to = ((y + dy) % 4) * 4 + (x + dx) % 4
            slot = tp_slot((4 - dy) % 4, (4 - dx) % 4)
            if l == 0:
                src, dst, recv = cur.at[1, 0], cur.at[1, slot], e_recv.at[0, slot // 4]
            else:
                src, dst, recv = final.at[h], final.at[h], e_recv.at[1, 0]
            remote(src, dst, e_send.at[l], recv, {"tp": to}).start()

    for l in range(2):
        wait_bytes(sq_pair_in.at[l], s1_send.at[l])
        wait_bytes(sq_in.at[l, pl.ds(0, 7)], s2_send.at[l])
        for half in range(2):
            wait_bytes(pair_in.at[l, pl.ds(0, 4)], a1_send.at[l, half])
        wait_bytes(sums_in.at[l, pl.ds(0, 7)], a2_send.at[l])
        wait_bytes(gat.at[l, pl.ds(0, 15)], c_send.at[l])
        wait_bytes(upd_in.at[l, pl.ds(0, 15)], d_send.at[l])
        wait_bytes(cur.at[0, pl.ds(0, 15)], e_send.at[l])
    wait_bytes(final.at[pl.ds(0, 15)], e_recv.at[1, 0])
    mixed_out[...] = final[...].reshape(256, 256)


def write_out(mixed, state, mixed_out, state_out, sem):
    copies = [pltpu.make_async_copy(mixed, mixed_out, sem.at[8])]
    for n in range(8):
        part = state.at[n // 4, pl.ds(4 * (n % 4), 4)]
        target = state_out.at[n // 4, pl.ds(4 * (n % 4), 4)]
        copies.append(pltpu.make_async_copy(part, target, sem.at[n]))
    for copy in copies:
        copy.start()
    for copy in copies:
        copy.wait()


def per_device(*args):
    any_spec = pl.BlockSpec(memory_space=pl.ANY)
    vmem_spec = pl.BlockSpec(memory_space=pltpu.VMEM)
    dma = pltpu.SemaphoreType.DMA
    shapes = ((256, 256), BF16), ((2, 16, 1, 128, 128), F32)
    held = pl.pallas_call(
        kernel,
        out_shape=tuple(pltpu.VMEM(shape, dtype) for shape, dtype in shapes),
        in_specs=[any_spec] * 10,
        out_specs=(vmem_spec, vmem_spec),
        scratch_shapes=[
            pltpu.VMEM((2, 16, 16, 256), BF16),
            pltpu.VMEM((2, 256), F32),
            pltpu.VMEM((2, 256, 512), BF16),
            pltpu.VMEM((2, 128), F32),
            pltpu.VMEM((2, 128), F32),
            pltpu.VMEM((2, 128, 256), BF16),
            pltpu.VMEM((2, 16, 128, 128), F32),
            pltpu.VMEM((2, 16, 16, 512), BF16),
            pltpu.VMEM((2, 8, 16, 512), BF16),
            pltpu.VMEM((2, 8, 16, 512), BF16),
            pltpu.VMEM((2, 8, 16, 512), BF16),
            pltpu.VMEM((2, 2, 1, 128), F32),
            pltpu.VMEM((2, 1, 128), F32),
            pltpu.VMEM((2, 1, 128), F32),
            pltpu.VMEM((2, 8, 1, 128), F32),
            pltpu.VMEM((2, 16, 16, 128), BF16),
            pltpu.VMEM((2, 16, 16, 256), BF16),
            pltpu.VMEM((2, 16, 16, 256), BF16),
            pltpu.VMEM((16, 16, 256), BF16),
            dma((17,)),
            dma,
            dma((2, 2)),
            dma((2, 2)),
            dma((2,)),
            dma((2,)),
            dma((2,)),
            dma((2,)),
            dma((2,)),
            dma((2,)),
            dma((2,)),
            dma((2, 3)),
            dma((2,)),
            dma((2,)),
            dma((2,)),
            dma((2, 4)),
        ],
        compiler_params=pltpu.CompilerParams(collective_id=0, has_side_effects=True),
    )(*args)
    return pl.pallas_call(
        write_out,
        out_shape=tuple(jax.ShapeDtypeStruct(shape, dtype) for shape, dtype in shapes),
        in_specs=[any_spec] * 2,
        out_specs=[any_spec] * 2,
        scratch_shapes=[dma((9,))],
        compiler_params=pltpu.CompilerParams(vmem_limit_bytes=1 << 20),
    )(*held)


def solution(mesh):
    in_specs = (
        P(None, "dp"),
        P(None, "dp"),
        P(None, "dp", "tp"),
        P(None, "dp", "tp"),
        P(None, "dp", "tp"),
        P(None, "dp", "tp"),
        P(None, "tp"),
        P(),
        P(None, "tp", "dp"),
        P(None, "dp", "tp", None, None),
    )
    out_specs = (P(None, "dp"), P(None, "dp", "tp", None, None))
    return jax.shard_map(
        per_device, mesh=mesh, in_specs=in_specs, out_specs=out_specs, check_vma=False
    )
```

```python
import functools

import jax
import jax.numpy as jnp
from jax import lax
from jax.experimental import pallas as pl
from jax.experimental.pallas import tpu as pltpu
from jax.sharding import PartitionSpec as P

D = 4096
DK = 128
EPS = 1e-06
MESH = pl.DeviceIdType.MESH
F32 = jnp.float32
BF16 = jnp.bfloat16

Z_ORDER = (0, 1, 7, 2, 6, 3, 5, 4)
C_GROUPS = ((0, 6), (6, 10), (10, 16))


def gray(v):
    return v + v // 2 - 2 * (v // 3)


def tp_slot(dy, dx):
    return (dx % 2) * 8 + (dx // 2) * 4 + gray(dy)


def z_slot(dz, rel):
    return 2 * Z_ORDER.index(dz) + rel


def z_slot_traced(dz, rel):
    pos = jnp.where(dz <= 4, 2 * dz - jnp.minimum(dz, 1), 16 - 2 * dz)
    return 2 * pos + rel


def kernel(
    tok_in,
    gain_in,
    wq_in,
    wf_in,
    wv_in,
    wg_in,
    floor_in,
    hgain_in,
    wout_in,
    state_in,
    mixed_out,
    state_out,
    cur,
    cur1,
    held,
    gain,
    gain1,
    w0,
    w1,
    floor,
    hgain,
    wout,
    old,
    part,
    pair_in,
    pair,
    sums_in,
    sq,
    sq_pair_in,
    sq_pair,
    sq_in,
    gat,
    upd,
    upd_in,
    final,
    load_sem,
    tok_sem,
    a1_send,
    a1_recv,
    s1_send,
    s1_recv,
    w1_send,
    w1_recv,
    g1_send,
    g1_recv,
    a2_send,
    a2_recv,
    s2_send,
    s2_recv,
    c_send,
    c_recv,
    d_send,
    d_recv,
    e_send,
    e_recv,
    e_send_pair,
    final_recv,
):
    h = lax.axis_index("tp")
    d = lax.axis_index("dp")
    y, x = h // 4, h % 4
    z, core = d // 2, d % 2
    e = (x + core) % 2
    partner = {"dp": 2 * z + 1 - core}

    toks = []
    for dy in range(4):
        for dx in range(4):
            rows = ((y + dy) % 4) * 4 + (x + dx) % 4
            copy = pltpu.make_async_copy(
                tok_in.at[pl.ds(rows * 16, 16), :], cur.at[tp_slot(dy, dx)], tok_sem
            )
            copy.start()
    tok_all = pltpu.make_async_copy(cur, cur, tok_sem)

    loads = {}

    def load(name, src, dst):
        loads[name] = pltpu.make_async_copy(src, dst, load_sem.at[len(loads)])
        loads[name].start()

    weights = (wq_in, wf_in, wv_in, wg_in)
    load("gain", gain_in, gain)
    for n in range(4):
        load(("w", 0, n), weights[n].at[0], w0.at[:, pl.ds(128 * n, 128)])
    barrier = pltpu.get_barrier_semaphore()
    for k in range(1, 16):
        to = (h + k) % 16
        pl.semaphore_signal(barrier, inc=1, device_id={"dp": (d + k) % 16}, device_id_type=MESH)
        pl.semaphore_signal(barrier, inc=1, device_id={"tp": to}, device_id_type=MESH)
        across = {"tp": to, **partner}
        pl.semaphore_signal(barrier, inc=1, device_id=across, device_id_type=MESH)

    own = pl.multiple_of(8 * e, 8)
    other = pl.multiple_of(8 - 8 * e, 8)
    self_dy = ((2 * z + core) // 4 - y + 4) % 4
    self_dx = ((2 * z + core) % 4 - x + 4) % 4
    self_slot = (self_dx // 2) * 4 + gray(self_dy)
    up_dz = (h // 2 - z + 8) % 8
    up_rel = (h % 2 + core) % 2
    up_slot = z_slot_traced(up_dz, up_rel)

    def remote(src, dst, send, recv, device):
        return pltpu.make_async_remote_copy(
            src_ref=src,
            dst_ref=dst,
            send_sem=send,
            recv_sem=recv,
            device_id=device,
            device_id_type=MESH,
        )

    def wait_bytes(ref, sem):
        pltpu.make_async_copy(ref, ref, sem).wait()

    def project(first, count):
        rows = cur[pl.ds(first, count)].astype(F32).reshape(16 * count, 256)
        normed = (rows * gain[0:1, :]).astype(BF16)
        product = jnp.dot(normed, w0[...], preferred_element_type=F32)
        part[pl.ds(first, count)] = product.astype(BF16).reshape(count, 16, 512)

    def squares(rows):
        ones = jnp.ones((8, rows.shape[1]), BF16)
        square = rows * rows
        high = square.astype(BF16)
        low = (square - high.astype(F32)).astype(BF16)
        dims = (((1,), (1,)), ((), ()))
        total = lax.dot_general(ones, high, dims, preferred_element_type=F32)
        total += lax.dot_general(ones, low, dims, preferred_element_type=F32)
        return total[:1]

    def send_along_z(l, i):
        block = ((y + gray(i % 4)) % 4) * 4 + (x + 2 * (i // 4) + e) % 4
        to_z = block // 2

        @pl.when(to_z != z)
        def _():
            remote(
                pair.at[l, i],
                sums_in.at[l, (z - to_z + 8) % 8],
                a2_send.at[l],
                a2_recv.at[l],
                {"dp": 2 * to_z + core},
            ).start()

    def send_squares_along_z(l):
        for k in range(1, 8):
            remote(
                sq_pair.at[l],
                sq_in.at[l, 8 - k],
                s2_send.at[l],
                s2_recv.at[l],
                {"dp": (d + 2 * k) % 16},
            ).start()

    for l in range(2):
        if l == 0:
            tok_all.wait()
            loads["gain"].wait()
            for n in range(4):
                loads["w", 0, n].wait()
            project(other, 8)
            load("floor", floor_in, floor)
            load("hgain", hgain_in, hgain)
            load(("state", 0), state_in.at[0, :, 0], old.at[0])
            load(("wout", 0), wout_in.at[0], wout.at[0])
            for n in range(4):
                load(("w", 1, n), weights[n].at[1], w1.at[core, :, pl.ds(128 * n, 128)])
            load(("state", 1), state_in.at[1, :, 0], old.at[1])
            load(("wout", 1), wout_in.at[1], wout.at[1])
            for c in range(2):
                sq[c] = squares(cur[8 * c : 8 * c + 8].astype(F32).reshape(128, 256))
            pl.semaphore_wait(barrier, 45)
            remote(sq.at[1 - e], sq_pair_in, s1_send, s1_recv, partner).start()
            for half in range(2):
                remote(
                    part.at[pl.ds(other + 4 * half, 4)],
                    pair_in.at[pl.ds(4 * half, 4)],
                    a1_send.at[half],
                    a1_recv.at[half],
                    partner,
                ).start()
            project(own, 8)
            wait_bytes(sq_pair_in, s1_recv)
            sq_pair[0] = sq[e] + sq_pair_in[...]
            send_squares_along_z(0)
            for half in range(2):
                wait_bytes(pair_in.at[pl.ds(0, 4)], a1_recv.at[half])
                mine = part[pl.ds(own + 4 * half, 4)].astype(F32)
                theirs = pair_in[4 * half : 4 * half + 4].astype(F32)
                pair[0, 4 * half : 4 * half + 4] = (mine + theirs).astype(BF16)
                for i in range(4):
                    send_along_z(0, 4 * half + i)
        else:
            wait_bytes(w1.at[0], w1_recv)
            wait_bytes(gain1.at[0], g1_recv)
            for half in range(2):
                wait_bytes(cur1.at[pl.ds(0, 4)], e_recv.at[half])
                rows = cur1[4 * half : 4 * half + 4].astype(F32).reshape(64, 512)
                normed = [(rows[:, 256 * c : 256 * c + 256] * gain1[c]).astype(BF16) for c in range(2)]
                product = jnp.dot(normed[0], w1[0], preferred_element_type=F32)
                product += jnp.dot(normed[1], w1[1], preferred_element_type=F32)
                pair[1, 4 * half : 4 * half + 4] = product.astype(BF16).reshape(4, 16, 512)
                for i in range(4):
                    send_along_z(1, 4 * half + i)
            sq_pair[1] = squares(cur1[...].astype(F32).reshape(128, 512))
            send_squares_along_z(1)

        wait_bytes(sq_in.at[l, pl.ds(0, 7)], s2_recv.at[l])
        row = sq_pair[l]
        for k in range(1, 8):
            row = row + sq_in[l, k]
        lanes = lax.broadcasted_iota(jnp.int32, (16, 128), 1)
        rows = lax.broadcasted_iota(jnp.int32, (16, 128), 0)
        picked = jnp.where(lanes == rows + 16 * self_slot, jnp.broadcast_to(row, (16, 128)), 0.0)
        row_scale = lax.rsqrt(jnp.sum(picked, axis=1, keepdims=True) / D + EPS)
        if l == 0:
            loads["floor"].wait()
            loads["hgain"].wait()
        loads["state", l].wait()
        wait_bytes(sums_in.at[l, pl.ds(0, 7)], a2_recv.at[l])
        total = pair[l, self_slot].astype(F32)
        for k in range(1, 8):
            total = total + sums_in[l, k].astype(F32)
        stored = (row_scale * total).astype(BF16).astype(F32)
        query_pre, forget_pre = stored[:, :128], stored[:, 128:256]
        value, gate_pre = stored[:, 256:384], stored[:, 384:]
        query = jax.nn.silu(query_pre) * DK ** (-0.5)
        low = floor[l : l + 1, :]
        forget = low + (1.0 - low) * jax.nn.sigmoid(forget_pre)
        key_in = (1.0 - low) * jax.nn.sigmoid(-forget_pre)
        scaled = (query * forget).T
        reads = []
        for b in range(16):
            reads.append(jnp.sum(old[l, b] * scaled[:, b : b + 1], axis=0, keepdims=True))
        read = jnp.concatenate(reads, axis=0)
        read = read + jnp.sum(query * key_in, axis=1, keepdims=True) * value
        read = read * lax.rsqrt(jnp.mean(read * read, axis=1, keepdims=True) + EPS)
        gated = read * hgain[l : l + 1, :] * jax.nn.silu(gate_pre)
        gat[l, 0] = gated.astype(BF16)

        for dz in reversed(Z_ORDER):
            for rel in (1, 0):
                if dz == 0 and rel == 0:
                    continue
                slot = z_slot((8 - dz) % 8, rel)
                to_core = core if rel == 0 else 1 - core
                group = [slot >= first and slot < last for first, last in C_GROUPS].index(True)
                remote(
                    gat.at[l, 0],
                    gat.at[l, slot],
                    c_send.at[l],
                    c_recv.at[l, group],
                    {"dp": 2 * ((z + dz) % 8) + to_core},
                ).start()

        if l == 0:
            for n in range(4):
                loads["w", 1, n].wait()
            remote(w1.at[core], w1.at[core], w1_send, w1_recv, partner).start()
            gain1[core] = gain[1:2, :]
            remote(gain1.at[core], gain1.at[core], g1_send, g1_recv, partner).start()

        forget_t, key_t = forget.T, key_in.T
        for b in range(16):
            kept = old[l, b] * forget_t[:, b : b + 1]
            state_out[l, b, 0] = kept + key_t[:, b : b + 1] * value[b : b + 1, :]

        loads["wout", l].wait()
        for group, (first, last) in enumerate(C_GROUPS):
            arrived = last - first - (1 if group == 0 else 0)
            wait_bytes(gat.at[l, pl.ds(0, arrived)], c_recv.at[l, group])
            rows = gat[l, first:last].reshape(16 * (last - first), 128)
            product = jnp.dot(rows, wout[l], preferred_element_type=F32)
            upd[l, first:last] = product.astype(BF16).reshape(last - first, 16, 256)
            for slot in range(first, last):
                dz, rel = Z_ORDER[slot // 2], slot % 2
                to_core = core if rel == 0 else 1 - core
                owner = 2 * ((z + dz) % 8) + to_core
                dy = (y - owner // 4 + 4) % 4
                dx = (x - owner % 4 + 4) % 4

                @pl.when(owner != h)
                def _():
                    remote(
                        upd.at[l, slot],
                        upd_in.at[l, tp_slot(dy, dx)],
                        d_send.at[l],
                        d_recv.at[l],
                        {"tp": owner},
                    ).start()

        wait_bytes(upd_in.at[l, pl.ds(0, 15)], d_recv.at[l])
        share = upd[l, up_slot].astype(F32)
        for s in range(1, 16):
            share = share + upd_in[l, s].astype(F32)
        before = cur[0] if l == 0 else held[...]
        fresh = (before.astype(F32) + share).astype(BF16)

        offsets = [(dy, dx) for dy in range(4) for dx in range(4) if dy or dx]
        near = (0, 1, 2, 1)
        offsets.sort(key=lambda o: -near[o[0]] - near[o[1]])
        if l == 0:
            held[...] = fresh
            to_core = x % 2
            for dy, dx in offsets:
                to = ((y + dy) % 4) * 4 + (x + dx) % 4
                slot = tp_slot((4 - dy) % 4, (4 - dx) % 4) % 8
                remote(
                    held,
                    cur1.at[slot, :, pl.ds(256 * core, 256)],
                    e_send.at[0],
                    e_recv.at[slot // 4],
                    {"tp": to, "dp": 2 * z + to_core},
                ).start()
            target = cur1.at[0, :, pl.ds(256 * core, 256)]

            @pl.when(to_core == core)
            def _():
                pltpu.make_async_copy(held, target, e_recv.at[0]).start()

            @pl.when(to_core != core)
            def _():
                remote(held, target, e_send_pair, e_recv.at[0], partner).start()
                wait_bytes(held, e_send_pair)
        else:
            final[h] = fresh
            for dy, dx in offsets:
                to = ((y + dy) % 4) * 4 + (x + dx) % 4
                remote(
                    final.at[h], final.at[h], e_send.at[1], final_recv, {"tp": to}
                ).start()

    wait_bytes(sq_pair_in, s1_send)
    for half in range(2):
        wait_bytes(pair_in.at[pl.ds(0, 4)], a1_send.at[half])
    wait_bytes(w1.at[0], w1_send)
    wait_bytes(gain1.at[0], g1_send)
    for l in range(2):
        wait_bytes(sq_in.at[l, pl.ds(0, 7)], s2_send.at[l])
        wait_bytes(sums_in.at[l, pl.ds(0, 7)], a2_send.at[l])
        wait_bytes(gat.at[l, pl.ds(0, 15)], c_send.at[l])
        wait_bytes(upd_in.at[l, pl.ds(0, 15)], d_send.at[l])
        wait_bytes(cur.at[pl.ds(0, 15)], e_send.at[l])
    wait_bytes(final.at[pl.ds(0, 15)], final_recv)
    mixed_out[...] = final[...].reshape(256, 256)


def write_out(mixed, state, mixed_out, state_out, sem):
    copies = [pltpu.make_async_copy(mixed, mixed_out, sem.at[8])]
    for n in range(8):
        part = state.at[n // 4, pl.ds(4 * (n % 4), 4)]
        target = state_out.at[n // 4, pl.ds(4 * (n % 4), 4)]
        copies.append(pltpu.make_async_copy(part, target, sem.at[n]))
    for copy in copies:
        copy.start()
    for copy in copies:
        copy.wait()


def per_device(*args):
    any_spec = pl.BlockSpec(memory_space=pl.ANY)
    vmem_spec = pl.BlockSpec(memory_space=pltpu.VMEM)
    dma = pltpu.SemaphoreType.DMA
    shapes = ((256, 256), BF16), ((2, 16, 1, 128, 128), F32)
    held = pl.pallas_call(
        kernel,
        out_shape=tuple(pltpu.VMEM(shape, dtype) for shape, dtype in shapes),
        in_specs=[any_spec] * 10,
        out_specs=(vmem_spec, vmem_spec),
        scratch_shapes=[
            pltpu.VMEM((16, 16, 256), BF16),
            pltpu.VMEM((8, 16, 512), BF16),
            pltpu.VMEM((16, 256), BF16),
            pltpu.VMEM((2, 256), F32),
            pltpu.VMEM((2, 1, 256), F32),
            pltpu.VMEM((256, 512), BF16),
            pltpu.VMEM((2, 256, 512), BF16),
            pltpu.VMEM((2, 128), F32),
            pltpu.VMEM((2, 128), F32),
            pltpu.VMEM((2, 128, 256), BF16),
            pltpu.VMEM((2, 16, 128, 128), F32),
            pltpu.VMEM((16, 16, 512), BF16),
            pltpu.VMEM((8, 16, 512), BF16),
            pltpu.VMEM((2, 8, 16, 512), BF16),
            pltpu.VMEM((2, 8, 16, 512), BF16),
            pltpu.VMEM((2, 1, 128), F32),
            pltpu.VMEM((1, 128), F32),
            pltpu.VMEM((2, 1, 128), F32),
            pltpu.VMEM((2, 8, 1, 128), F32),
            pltpu.VMEM((2, 16, 16, 128), BF16),
            pltpu.VMEM((2, 16, 16, 256), BF16),
            pltpu.VMEM((2, 16, 16, 256), BF16),
            pltpu.VMEM((16, 16, 256), BF16),
            dma((17,)),
            dma,
            dma((2,)),
            dma((2,)),
            dma,
            dma,
            dma,
            dma,
            dma,
            dma,
            dma((2,)),
            dma((2,)),
            dma((2,)),
            dma((2,)),
            dma((2,)),
            dma((2, 3)),
            dma((2,)),
            dma((2,)),
            dma((2,)),
            dma((2,)),
            dma,
            dma,
        ],
        compiler_params=pltpu.CompilerParams(collective_id=0, has_side_effects=True),
    )(*args)
    return pl.pallas_call(
        write_out,
        out_shape=tuple(jax.ShapeDtypeStruct(shape, dtype) for shape, dtype in shapes),
        in_specs=[any_spec] * 2,
        out_specs=[any_spec] * 2,
        scratch_shapes=[dma((9,))],
        compiler_params=pltpu.CompilerParams(vmem_limit_bytes=1 << 20),
    )(*held)


def solution(mesh):
    in_specs = (
        P(None, "dp"),
        P(None, "dp"),
        P(None, "dp", "tp"),
        P(None, "dp", "tp"),
        P(None, "dp", "tp"),
        P(None, "dp", "tp"),
        P(None, "tp"),
        P(),
        P(None, "tp", "dp"),
        P(None, "dp", "tp", None, None),
    )
    out_specs = (P(None, "dp"), P(None, "dp", "tp", None, None))
    return jax.shard_map(
        per_device, mesh=mesh, in_specs=in_specs, out_specs=out_specs, check_vma=False
    )
```

```python
import functools

import jax
import jax.numpy as jnp
from jax import lax
from jax.experimental import pallas as pl
from jax.experimental.pallas import tpu as pltpu
from jax.sharding import PartitionSpec as P

D = 4096
DK = 128
EPS = 1e-06
MESH = pl.DeviceIdType.MESH
F32 = jnp.float32
BF16 = jnp.bfloat16

Z_FAR = (4, 3, 5, 2, 6, 1, 7, 0)
TP_GROUPS = (0, 2, 3, 1)


def gray(v):
    return v + v // 2 - 2 * (v // 3)


def tp_slot(dy, dx):
    return (dx % 2) * 8 + (dx // 2) * 4 + gray(dy)


def kernel(
    tok_in,
    gain_in,
    wq_in,
    wf_in,
    wv_in,
    wg_in,
    floor_in,
    hgain_in,
    wout_in,
    state_in,
    mixed_out,
    state_out,
    cur,
    cur1,
    held,
    gain,
    gain1,
    w0,
    w1,
    floor,
    hgain,
    wout,
    old,
    part,
    pair_in,
    pair,
    sums_in,
    sq,
    sq_pair_in,
    sq_pair,
    sq_in,
    gat,
    gat_in,
    final,
    load_sem,
    tok_sem,
    a1_send,
    a1_recv,
    s1_send,
    s1_recv,
    w1_send,
    w1_recv,
    g1_send,
    g1_recv,
    a2_send,
    a2_recv,
    s2_send,
    s2_recv,
    c_send,
    c_recv,
    o_send,
    o_recv,
    e_send,
    e_recv,
    e_send_pair,
    final_recv,
):
    h = lax.axis_index("tp")
    d = lax.axis_index("dp")
    y, x = h // 4, h % 4
    z, core = d // 2, d % 2
    e = (x + core) % 2
    partner = {"dp": 2 * z + 1 - core}

    toks = []
    for dy in range(4):
        for dx in range(4):
            rows = ((y + dy) % 4) * 4 + (x + dx) % 4
            copy = pltpu.make_async_copy(
                tok_in.at[pl.ds(rows * 16, 16), :], cur.at[tp_slot(dy, dx)], tok_sem
            )
            copy.start()
    tok_all = pltpu.make_async_copy(cur, cur, tok_sem)

    loads = {}

    def load(name, src, dst):
        loads[name] = pltpu.make_async_copy(src, dst, load_sem.at[len(loads)])
        loads[name].start()

    weights = (wq_in, wf_in, wv_in, wg_in)
    load("gain", gain_in, gain)
    for n in range(4):
        load(("w", 0, n), weights[n].at[0], w0.at[:, pl.ds(128 * n, 128)])
    barrier = pltpu.get_barrier_semaphore()
    for k in range(1, 16):
        to = (h + k) % 16
        pl.semaphore_signal(barrier, inc=1, device_id={"dp": (d + k) % 16}, device_id_type=MESH)
        pl.semaphore_signal(barrier, inc=1, device_id={"tp": to}, device_id_type=MESH)
        across = {"tp": to, **partner}
        pl.semaphore_signal(barrier, inc=1, device_id=across, device_id_type=MESH)
        away = {"tp": to, "dp": h}
        pl.semaphore_signal(barrier, inc=1, device_id=away, device_id_type=MESH)

    @pl.when(h != d)
    def _():
        pl.semaphore_signal(barrier, inc=1, device_id={"dp": h}, device_id_type=MESH)


    own = pl.multiple_of(8 * e, 8)
    other = pl.multiple_of(8 - 8 * e, 8)
    self_dy = ((2 * z + core) // 4 - y + 4) % 4
    self_dx = ((2 * z + core) % 4 - x + 4) % 4
    self_slot = (self_dx // 2) * 4 + gray(self_dy)
    own_slot = tp_slot((y - d // 4 + 4) % 4, (x - d % 4 + 4) % 4)
    near = (0, 1, 2, 1)
    offsets = [(dy, dx) for dy in range(4) for dx in range(4) if dy or dx]
    offsets.sort(key=lambda o: -near[o[0]] - near[o[1]])
    peers = [
        (((y + dy) % 4) * 4 + (x + dx) % 4, tp_slot((4 - dy) % 4, (4 - dx) % 4)) for dy, dx in offsets
    ]

    def remote(src, dst, send, recv, device):
        return pltpu.make_async_remote_copy(
            src_ref=src,
            dst_ref=dst,
            send_sem=send,
            recv_sem=recv,
            device_id=device,
            device_id_type=MESH,
        )

    def wait_bytes(ref, sem):
        pltpu.make_async_copy(ref, ref, sem).wait()

    def project(first, count):
        rows = cur[pl.ds(first, count)].astype(F32).reshape(16 * count, 256)
        normed = (rows * gain[0:1, :]).astype(BF16)
        product = jnp.dot(normed, w0[...], preferred_element_type=F32)
        part[pl.ds(first, count)] = product.astype(BF16).reshape(count, 16, 512)

    def squares(rows):
        ones = jnp.ones((8, rows.shape[1]), BF16)
        square = rows * rows
        high = square.astype(BF16)
        low = (square - high.astype(F32)).astype(BF16)
        dims = (((1,), (1,)), ((), ()))
        total = lax.dot_general(ones, high, dims, preferred_element_type=F32)
        total += lax.dot_general(ones, low, dims, preferred_element_type=F32)
        return total[:1]

    def send_along_z(l, i):
        block = ((y + gray(i % 4)) % 4) * 4 + (x + 2 * (i // 4) + e) % 4
        to_z = block // 2

        @pl.when(to_z != z)
        def _():
            remote(
                pair.at[l, i],
                sums_in.at[l, (z - to_z + 8) % 8],
                a2_send.at[l],
                a2_recv.at[l],
                {"dp": 2 * to_z + core},
            ).start()

    def send_squares_along_z(l):
        for k in range(1, 8):
            remote(
                sq_pair.at[l],
                sq_in.at[l, 8 - k],
                s2_send.at[l],
                s2_recv.at[l],
                {"dp": (d + 2 * k) % 16},
            ).start()

    def gather_weights(l):
        loads["wout", l].wait()
        for to, slot in peers:
            remote(
                wout.at[l, 0], wout.at[l, slot], o_send.at[l], o_recv.at[l], {"tp": to}
            ).start()

    for l in range(2):
        if l == 0:
            tok_all.wait()
            loads["gain"].wait()
            for n in range(4):
                loads["w", 0, n].wait()
            project(other, 8)
            load("floor", floor_in, floor)
            load("hgain", hgain_in, hgain)
            load(("state", 0), state_in.at[0, :, 0], old.at[0])
            load(("wout", 0), wout_in.at[0], wout.at[0, 0])
            for n in range(4):
                load(("w", 1, n), weights[n].at[1], w1.at[core, :, pl.ds(128 * n, 128)])
            load(("state", 1), state_in.at[1, :, 0], old.at[1])
            load(("wout", 1), wout_in.at[1], wout.at[1, 0])
            for c in range(2):
                sq[c] = squares(cur[8 * c : 8 * c + 8].astype(F32).reshape(128, 256))
            pl.semaphore_wait(barrier, jnp.where(h == d, 60, 61))
            remote(sq.at[1 - e], sq_pair_in, s1_send, s1_recv, partner).start()
            for half in range(2):
                remote(
                    part.at[pl.ds(other + 4 * half, 4)],
                    pair_in.at[pl.ds(4 * half, 4)],
                    a1_send.at[half],
                    a1_recv.at[half],
                    partner,
                ).start()
            project(own, 8)
            wait_bytes(sq_pair_in, s1_recv)
            sq_pair[0] = sq[e] + sq_pair_in[...]
            send_squares_along_z(0)
            for half in range(2):
                wait_bytes(pair_in.at[pl.ds(0, 4)], a1_recv.at[half])
                mine = part[pl.ds(own + 4 * half, 4)].astype(F32)
                theirs = pair_in[4 * half : 4 * half + 4].astype(F32)
                pair[0, 4 * half : 4 * half + 4] = (mine + theirs).astype(BF16)
                for i in range(4):
                    send_along_z(0, 4 * half + i)
            gather_weights(0)
        else:
            wait_bytes(w1.at[0], w1_recv)
            wait_bytes(gain1.at[0], g1_recv)
            for half in range(2):
                wait_bytes(cur1.at[pl.ds(0, 4)], e_recv.at[half])
                rows = cur1[4 * half : 4 * half + 4].astype(F32).reshape(64, 512)
                normed = [(rows[:, 256 * c : 256 * c + 256] * gain1[c]).astype(BF16) for c in range(2)]
                product = jnp.dot(normed[0], w1[0], preferred_element_type=F32)
                product += jnp.dot(normed[1], w1[1], preferred_element_type=F32)
                pair[1, 4 * half : 4 * half + 4] = product.astype(BF16).reshape(4, 16, 512)
                for i in range(4):
                    send_along_z(1, 4 * half + i)
            sq_pair[1] = squares(cur1[...].astype(F32).reshape(128, 512))
            send_squares_along_z(1)

        wait_bytes(sq_in.at[l, pl.ds(0, 7)], s2_recv.at[l])
        row = sq_pair[l]
        for k in range(1, 8):
            row = row + sq_in[l, k]
        lanes = lax.broadcasted_iota(jnp.int32, (16, 128), 1)
        rows = lax.broadcasted_iota(jnp.int32, (16, 128), 0)
        picked = jnp.where(lanes == rows + 16 * self_slot, jnp.broadcast_to(row, (16, 128)), 0.0)
        row_scale = lax.rsqrt(jnp.sum(picked, axis=1, keepdims=True) / D + EPS)
        if l == 0:
            loads["floor"].wait()
            loads["hgain"].wait()
        loads["state", l].wait()
        wait_bytes(sums_in.at[l, pl.ds(0, 7)], a2_recv.at[l])
        total = pair[l, self_slot].astype(F32)
        for k in range(1, 8):
            total = total + sums_in[l, k].astype(F32)
        stored = (row_scale * total).astype(BF16).astype(F32)
        query_pre, forget_pre = stored[:, :128], stored[:, 128:256]
        value, gate_pre = stored[:, 256:384], stored[:, 384:]
        query = jax.nn.silu(query_pre) * DK ** (-0.5)
        low = floor[l : l + 1, :]
        forget = low + (1.0 - low) * jax.nn.sigmoid(forget_pre)
        key_in = (1.0 - low) * jax.nn.sigmoid(-forget_pre)
        scaled = (query * forget).T
        reads = []
        for b in range(16):
            reads.append(jnp.sum(old[l, b] * scaled[:, b : b + 1], axis=0, keepdims=True))
        read = jnp.concatenate(reads, axis=0)
        read = read + jnp.sum(query * key_in, axis=1, keepdims=True) * value
        read = read * lax.rsqrt(jnp.mean(read * read, axis=1, keepdims=True) + EPS)
        gated = read * hgain[l : l + 1, :] * jax.nn.silu(gate_pre)
        gat[l] = gated.astype(BF16)

        landing = gat_in.at[l, own_slot]
        recv = c_recv.at[l, own_slot // 4]
        for dz in Z_FAR:
            for other_core in (1, 0):
                to = 2 * ((z + dz) % 8) + (core + other_core) % 2

                @pl.when((h != d) | (to != d))
                def _():
                    remote(
                        gat.at[l], landing, c_send.at[l], recv, {"tp": d, "dp": to}
                    ).start()

        @pl.when(h == d)
        def _():
            pltpu.make_async_copy(gat.at[l], landing, recv).start()

        if l == 0:
            for n in range(4):
                loads["w", 1, n].wait()
            remote(w1.at[core], w1.at[core], w1_send, w1_recv, partner).start()
            gain1[core] = gain[1:2, :]
            remote(gain1.at[core], gain1.at[core], g1_send, g1_recv, partner).start()

        forget_t, key_t = forget.T, key_in.T
        for b in range(16):
            kept = old[l, b] * forget_t[:, b : b + 1]
            state_out[l, b, 0] = kept + key_t[:, b : b + 1] * value[b : b + 1, :]

        wait_bytes(wout.at[l, pl.ds(0, 15)], o_recv.at[l])
        share = jnp.zeros((16, 256), F32)
        for group in TP_GROUPS:
            wait_bytes(gat_in.at[l, pl.ds(0, 4)], c_recv.at[l, group])
            heads = [gat_in[l, 4 * group + i] for i in range(4)]
            rows = jnp.concatenate(heads, axis=1)
            columns = wout[l, 4 * group : 4 * group + 4].reshape(512, 256)
            share += jnp.dot(rows, columns, preferred_element_type=F32)
        before = cur[0] if l == 0 else held[...]
        fresh = (before.astype(F32) + share).astype(BF16)

        if l == 0:
            held[...] = fresh
            to_core = x % 2
            for to, tp_slot_there in peers:
                slot = tp_slot_there % 8
                remote(
                    held,
                    cur1.at[slot, :, pl.ds(256 * core, 256)],
                    e_send.at[0],
                    e_recv.at[slot // 4],
                    {"tp": to, "dp": 2 * z + to_core},
                ).start()
            target = cur1.at[0, :, pl.ds(256 * core, 256)]

            @pl.when(to_core == core)
            def _():
                pltpu.make_async_copy(held, target, e_recv.at[0]).start()

            @pl.when(to_core != core)
            def _():
                remote(held, target, e_send_pair, e_recv.at[0], partner).start()
                wait_bytes(held, e_send_pair)

            gather_weights(1)
        else:
            final[h] = fresh
            for to, _ in peers:
                remote(
                    final.at[h], final.at[h], e_send.at[1], final_recv, {"tp": to}
                ).start()

    wait_bytes(sq_pair_in, s1_send)
    for half in range(2):
        wait_bytes(pair_in.at[pl.ds(0, 4)], a1_send.at[half])
    wait_bytes(w1.at[0], w1_send)
    wait_bytes(gain1.at[0], g1_send)
    for l in range(2):
        wait_bytes(sq_in.at[l, pl.ds(0, 7)], s2_send.at[l])
        wait_bytes(sums_in.at[l, pl.ds(0, 7)], a2_send.at[l])
        wait_bytes(wout.at[l, pl.ds(0, 15)], o_send.at[l])

        @pl.when(h == d)
        def _():
            wait_bytes(gat_in.at[l, pl.ds(0, 15)], c_send.at[l])

        @pl.when(h != d)
        def _():
            wait_bytes(gat_in.at[l], c_send.at[l])

        wait_bytes(cur.at[pl.ds(0, 15)], e_send.at[l])
    wait_bytes(final.at[pl.ds(0, 15)], final_recv)
    mixed_out[...] = final[...].reshape(256, 256)


def write_out(mixed, state, mixed_out, state_out, sem):
    copies = [pltpu.make_async_copy(mixed, mixed_out, sem.at[8])]
    for n in range(8):
        part = state.at[n // 4, pl.ds(4 * (n % 4), 4)]
        target = state_out.at[n // 4, pl.ds(4 * (n % 4), 4)]
        copies.append(pltpu.make_async_copy(part, target, sem.at[n]))
    for copy in copies:
        copy.start()
    for copy in copies:
        copy.wait()


def per_device(*args):
    any_spec = pl.BlockSpec(memory_space=pl.ANY)
    vmem_spec = pl.BlockSpec(memory_space=pltpu.VMEM)
    dma = pltpu.SemaphoreType.DMA
    shapes = ((256, 256), BF16), ((2, 16, 1, 128, 128), F32)
    held = pl.pallas_call(
        kernel,
        out_shape=tuple(pltpu.VMEM(shape, dtype) for shape, dtype in shapes),
        in_specs=[any_spec] * 10,
        out_specs=(vmem_spec, vmem_spec),
        scratch_shapes=[
            pltpu.VMEM((16, 16, 256), BF16),
            pltpu.VMEM((8, 16, 512), BF16),
            pltpu.VMEM((16, 256), BF16),
            pltpu.VMEM((2, 256), F32),
            pltpu.VMEM((2, 1, 256), F32),
            pltpu.VMEM((256, 512), BF16),
            pltpu.VMEM((2, 256, 512), BF16),
            pltpu.VMEM((2, 128), F32),
            pltpu.VMEM((2, 128), F32),
            pltpu.VMEM((2, 16, 128, 256), BF16),
            pltpu.VMEM((2, 16, 128, 128), F32),
            pltpu.VMEM((16, 16, 512), BF16),
            pltpu.VMEM((8, 16, 512), BF16),
            pltpu.VMEM((2, 8, 16, 512), BF16),
            pltpu.VMEM((2, 8, 16, 512), BF16),
            pltpu.VMEM((2, 1, 128), F32),
            pltpu.VMEM((1, 128), F32),
            pltpu.VMEM((2, 1, 128), F32),
            pltpu.VMEM((2, 8, 1, 128), F32),
            pltpu.VMEM((2, 16, 128), BF16),
            pltpu.VMEM((2, 16, 16, 128), BF16),
            pltpu.VMEM((16, 16, 256), BF16),
            dma((17,)),
            dma,
            dma((2,)),
            dma((2,)),
            dma,
            dma,
            dma,
            dma,
            dma,
            dma,
            dma((2,)),
            dma((2,)),
            dma((2,)),
            dma((2,)),
            dma((2,)),
            dma((2, 4)),
            dma((2,)),
            dma((2,)),
            dma((2,)),
            dma((2,)),
            dma,
            dma,
        ],
        compiler_params=pltpu.CompilerParams(collective_id=0, has_side_effects=True),
    )(*args)
    return pl.pallas_call(
        write_out,
        out_shape=tuple(jax.ShapeDtypeStruct(shape, dtype) for shape, dtype in shapes),
        in_specs=[any_spec] * 2,
        out_specs=[any_spec] * 2,
        scratch_shapes=[dma((9,))],
        compiler_params=pltpu.CompilerParams(vmem_limit_bytes=1 << 20),
    )(*held)


def solution(mesh):
    in_specs = (
        P(None, "dp"),
        P(None, "dp"),
        P(None, "dp", "tp"),
        P(None, "dp", "tp"),
        P(None, "dp", "tp"),
        P(None, "dp", "tp"),
        P(None, "tp"),
        P(),
        P(None, "tp", "dp"),
        P(None, "dp", "tp", None, None),
    )
    out_specs = (P(None, "dp"), P(None, "dp", "tp", None, None))
    return jax.shard_map(
        per_device, mesh=mesh, in_specs=in_specs, out_specs=out_specs, check_vma=False
    )
```

```python
import functools

import jax
import jax.numpy as jnp
from jax import lax
from jax.experimental import pallas as pl
from jax.experimental.pallas import tpu as pltpu
from jax.sharding import PartitionSpec as P

D = 4096
DK = 128
EPS = 1e-06
MESH = pl.DeviceIdType.MESH
F32 = jnp.float32
BF16 = jnp.bfloat16

Z_FAR = (4, 3, 5, 2, 6, 1, 7, 0)
TP_GROUPS = (0, 2, 3, 1)


def gray(v):
    return v + v // 2 - 2 * (v // 3)


def tp_slot(dy, dx):
    return (dx % 2) * 8 + (dx // 2) * 4 + gray(dy)


def kernel(
    tok_in,
    gain_in,
    wq_in,
    wf_in,
    wv_in,
    wg_in,
    floor_in,
    hgain_in,
    wout_in,
    state_in,
    mixed_out,
    state_out,
    cur,
    cur1,
    held,
    gain,
    gain1,
    w0,
    w1,
    floor,
    hgain,
    wout,
    old,
    part,
    pair_in,
    pair,
    sums_in,
    sq,
    sq_pair_in,
    sq_pair,
    sq_in,
    gat,
    gat_in,
    final,
    load_sem,
    tok_sem,
    a1_send,
    a1_recv,
    s1_send,
    s1_recv,
    w1_send,
    w1_recv,
    g1_send,
    g1_recv,
    a2_send,
    a2_recv,
    s2_send,
    s2_recv,
    c_send,
    c_recv,
    ox_send,
    ox_recv,
    oy_send,
    oy_recv,
    e_send,
    e_recv,
    e_send_pair,
    final_recv,
):
    h = lax.axis_index("tp")
    d = lax.axis_index("dp")
    y, x = h // 4, h % 4
    z, core = d // 2, d % 2
    e = (x + core) % 2
    partner = {"dp": 2 * z + 1 - core}

    toks = []
    for dy in range(4):
        for dx in range(4):
            rows = ((y + dy) % 4) * 4 + (x + dx) % 4
            copy = pltpu.make_async_copy(
                tok_in.at[pl.ds(rows * 16, 16), :], cur.at[tp_slot(dy, dx)], tok_sem
            )
            copy.start()
    tok_all = pltpu.make_async_copy(cur, cur, tok_sem)

    loads = {}

    def load(name, src, dst):
        loads[name] = pltpu.make_async_copy(src, dst, load_sem.at[len(loads)])
        loads[name].start()

    weights = (wq_in, wf_in, wv_in, wg_in)
    load("gain", gain_in, gain)
    for n in range(4):
        load(("w", 0, n), weights[n].at[0], w0.at[:, pl.ds(128 * n, 128)])
    barrier = pltpu.get_barrier_semaphore()
    for k in range(1, 16):
        to = (h + k) % 16
        pl.semaphore_signal(barrier, inc=1, device_id={"dp": (d + k) % 16}, device_id_type=MESH)
        pl.semaphore_signal(barrier, inc=1, device_id={"tp": to}, device_id_type=MESH)
        across = {"tp": to, **partner}
        pl.semaphore_signal(barrier, inc=1, device_id=across, device_id_type=MESH)
        away = {"tp": to, "dp": h}
        pl.semaphore_signal(barrier, inc=1, device_id=away, device_id_type=MESH)

    @pl.when(h != d)
    def _():
        pl.semaphore_signal(barrier, inc=1, device_id={"dp": h}, device_id_type=MESH)


    own = pl.multiple_of(8 * e, 8)
    other = pl.multiple_of(8 - 8 * e, 8)
    self_dy = ((2 * z + core) // 4 - y + 4) % 4
    self_dx = ((2 * z + core) % 4 - x + 4) % 4
    self_slot = (self_dx // 2) * 4 + gray(self_dy)
    own_slot = tp_slot((y - d // 4 + 4) % 4, (x - d % 4 + 4) % 4)
    near = (0, 1, 2, 1)
    offsets = [(dy, dx) for dy in range(4) for dx in range(4) if dy or dx]
    offsets.sort(key=lambda o: -near[o[0]] - near[o[1]])
    peers = [
        (((y + dy) % 4) * 4 + (x + dx) % 4, tp_slot((4 - dy) % 4, (4 - dx) % 4)) for dy, dx in offsets
    ]

    def remote(src, dst, send, recv, device):
        return pltpu.make_async_remote_copy(
            src_ref=src,
            dst_ref=dst,
            send_sem=send,
            recv_sem=recv,
            device_id=device,
            device_id_type=MESH,
        )

    def wait_bytes(ref, sem):
        pltpu.make_async_copy(ref, ref, sem).wait()

    def project(first, count):
        rows = cur[pl.ds(first, count)].astype(F32).reshape(16 * count, 256)
        normed = (rows * gain[0:1, :]).astype(BF16)
        product = jnp.dot(normed, w0[...], preferred_element_type=F32)
        part[pl.ds(first, count)] = product.astype(BF16).reshape(count, 16, 512)

    def squares(rows):
        ones = jnp.ones((8, rows.shape[1]), BF16)
        square = rows * rows
        high = square.astype(BF16)
        low = (square - high.astype(F32)).astype(BF16)
        dims = (((1,), (1,)), ((), ()))
        total = lax.dot_general(ones, high, dims, preferred_element_type=F32)
        total += lax.dot_general(ones, low, dims, preferred_element_type=F32)
        return total[:1]

    def send_along_z(l, i):
        block = ((y + gray(i % 4)) % 4) * 4 + (x + 2 * (i // 4) + e) % 4
        to_z = block // 2

        @pl.when(to_z != z)
        def _():
            remote(
                pair.at[l, i],
                sums_in.at[l, (z - to_z + 8) % 8],
                a2_send.at[l],
                a2_recv.at[l],
                {"dp": 2 * to_z + core},
            ).start()

    def send_squares_along_z(l):
        for k in range(1, 8):
            remote(
                sq_pair.at[l],
                sq_in.at[l, 8 - k],
                s2_send.at[l],
                s2_recv.at[l],
                {"dp": (d + 2 * k) % 16},
            ).start()

    def along_x(dx):
        return {"tp": y * 4 + (x + dx) % 4}

    def along_y(dy):
        return {"tp": ((y + dy) % 4) * 4 + x}

    upper, lower = pl.ds(0, 64), pl.ds(64, 64)

    def gather_first(l):
        loads["wout", l].wait()
        for n in (2, 1, 3):
            there = tp_slot(0, 4 - n) // 4
            src, dst = wout.at[l, 0, 0, upper], wout.at[l, there, 0, upper]
            remote(src, dst, ox_send.at[l, 0], ox_recv.at[l, 0], along_x(n)).start()
            src, dst = wout.at[l, 0, 0, lower], wout.at[l, 0, gray(4 - n), lower]
            remote(src, dst, oy_send.at[l, 0], oy_recv.at[l, 0], along_y(n)).start()

    def gather_second(l):
        wait_bytes(wout.at[l, 0, pl.ds(0, 3), upper], ox_recv.at[l, 0])
        wait_bytes(wout.at[l, 0, pl.ds(0, 3), lower], oy_recv.at[l, 0])
        for n in (2, 1, 3):
            src, dst = wout.at[l, :, 0, upper], wout.at[l, :, gray(4 - n), upper]
            remote(src, dst, oy_send.at[l, 1], oy_recv.at[l, 1], along_y(n)).start()
            there = tp_slot(0, 4 - n) // 4
            src, dst = wout.at[l, 0, :, lower], wout.at[l, there, :, lower]
            remote(src, dst, ox_send.at[l, 1], ox_recv.at[l, 1], along_x(n)).start()

    for l in range(2):
        if l == 0:
            tok_all.wait()
            loads["gain"].wait()
            for n in range(4):
                loads["w", 0, n].wait()
            project(other, 8)
            load("floor", floor_in, floor)
            load("hgain", hgain_in, hgain)
            load(("state", 0), state_in.at[0, :, 0], old.at[0])
            load(("wout", 0), wout_in.at[0], wout.at[0, 0, 0])
            for n in range(4):
                load(("w", 1, n), weights[n].at[1], w1.at[core, :, pl.ds(128 * n, 128)])
            load(("state", 1), state_in.at[1, :, 0], old.at[1])
            load(("wout", 1), wout_in.at[1], wout.at[1, 0, 0])
            for c in range(2):
                sq[c] = squares(cur[8 * c : 8 * c + 8].astype(F32).reshape(128, 256))
            pl.semaphore_wait(barrier, jnp.where(h == d, 60, 61))
            remote(sq.at[1 - e], sq_pair_in, s1_send, s1_recv, partner).start()
            for half in range(2):
                remote(
                    part.at[pl.ds(other + 4 * half, 4)],
                    pair_in.at[pl.ds(4 * half, 4)],
                    a1_send.at[half],
                    a1_recv.at[half],
                    partner,
                ).start()
            gather_first(0)
            project(own, 8)
            wait_bytes(sq_pair_in, s1_recv)
            sq_pair[0] = sq[e] + sq_pair_in[...]
            send_squares_along_z(0)
            for half in range(2):
                wait_bytes(pair_in.at[pl.ds(0, 4)], a1_recv.at[half])
                mine = part[pl.ds(own + 4 * half, 4)].astype(F32)
                theirs = pair_in[4 * half : 4 * half + 4].astype(F32)
                pair[0, 4 * half : 4 * half + 4] = (mine + theirs).astype(BF16)
                for i in range(4):
                    send_along_z(0, 4 * half + i)
        else:
            wait_bytes(w1.at[0], w1_recv)
            wait_bytes(gain1.at[0], g1_recv)
            for half in range(2):
                wait_bytes(cur1.at[pl.ds(0, 4)], e_recv.at[half])
                if half == 1:
                    sq_pair[1] = squares(cur1[...].astype(F32).reshape(128, 512))
                    send_squares_along_z(1)
                rows = cur1[4 * half : 4 * half + 4].astype(F32).reshape(64, 512)
                normed = [(rows[:, 256 * c : 256 * c + 256] * gain1[c]).astype(BF16) for c in range(2)]
                product = jnp.dot(normed[0], w1[0], preferred_element_type=F32)
                product += jnp.dot(normed[1], w1[1], preferred_element_type=F32)
                pair[1, 4 * half : 4 * half + 4] = product.astype(BF16).reshape(4, 16, 512)
                for i in range(4):
                    send_along_z(1, 4 * half + i)
        gather_second(l)

        wait_bytes(sq_in.at[l, pl.ds(0, 7)], s2_recv.at[l])
        row = sq_pair[l]
        for k in range(1, 8):
            row = row + sq_in[l, k]
        lanes = lax.broadcasted_iota(jnp.int32, (16, 128), 1)
        rows = lax.broadcasted_iota(jnp.int32, (16, 128), 0)
        picked = jnp.where(lanes == rows + 16 * self_slot, jnp.broadcast_to(row, (16, 128)), 0.0)
        row_scale = lax.rsqrt(jnp.sum(picked, axis=1, keepdims=True) / D + EPS)
        if l == 0:
            loads["floor"].wait()
            loads["hgain"].wait()
        loads["state", l].wait()
        wait_bytes(sums_in.at[l, pl.ds(0, 7)], a2_recv.at[l])
        total = pair[l, self_slot].astype(F32)
        for k in range(1, 8):
            total = total + sums_in[l, k].astype(F32)
        stored = (row_scale * total).astype(BF16).astype(F32)
        query_pre, forget_pre = stored[:, :128], stored[:, 128:256]
        value, gate_pre = stored[:, 256:384], stored[:, 384:]
        query = jax.nn.silu(query_pre) * DK ** (-0.5)
        low = floor[l : l + 1, :]
        forget = low + (1.0 - low) * jax.nn.sigmoid(forget_pre)
        key_in = (1.0 - low) * jax.nn.sigmoid(-forget_pre)
        scaled = (query * forget).T
        reads = []
        for b in range(16):
            reads.append(jnp.sum(old[l, b] * scaled[:, b : b + 1], axis=0, keepdims=True))
        read = jnp.concatenate(reads, axis=0)
        read = read + jnp.sum(query * key_in, axis=1, keepdims=True) * value
        read = read * lax.rsqrt(jnp.mean(read * read, axis=1, keepdims=True) + EPS)
        gated = read * hgain[l : l + 1, :] * jax.nn.silu(gate_pre)
        gat[l] = gated.astype(BF16)

        landing = gat_in.at[l, own_slot]
        recv = c_recv.at[l, own_slot // 4]
        for dz in Z_FAR:
            for other_core in (1, 0):
                to = 2 * ((z + dz) % 8) + (core + other_core) % 2

                @pl.when((h != d) | (to != d))
                def _():
                    remote(
                        gat.at[l], landing, c_send.at[l], recv, {"tp": d, "dp": to}
                    ).start()

        @pl.when(h == d)
        def _():
            pltpu.make_async_copy(gat.at[l], landing, recv).start()

        if l == 0:
            for n in range(4):
                loads["w", 1, n].wait()
            remote(w1.at[core], w1.at[core], w1_send, w1_recv, partner).start()
            gain1[core] = gain[1:2, :]
            remote(gain1.at[core], gain1.at[core], g1_send, g1_recv, partner).start()

        forget_t, key_t = forget.T, key_in.T
        for b in range(16):
            kept = old[l, b] * forget_t[:, b : b + 1]
            state_out[l, b, 0] = kept + key_t[:, b : b + 1] * value[b : b + 1, :]

        if l == 0:
            gather_first(1)

        wait_bytes(wout.at[l, pl.ds(0, 3), :, upper], oy_recv.at[l, 1])
        wait_bytes(wout.at[l, pl.ds(0, 3), :, lower], ox_recv.at[l, 1])
        share = jnp.zeros((16, 256), F32)
        for group in TP_GROUPS:
            wait_bytes(gat_in.at[l, pl.ds(0, 4)], c_recv.at[l, group])
            heads = [gat_in[l, 4 * group + i] for i in range(4)]
            rows = jnp.concatenate(heads, axis=1)
            columns = wout[l, group].reshape(512, 256)
            share += jnp.dot(rows, columns, preferred_element_type=F32)
        before = cur[0] if l == 0 else held[...]
        fresh = (before.astype(F32) + share).astype(BF16)

        if l == 0:
            held[...] = fresh
            to_core = x % 2
            for to, tp_slot_there in peers:
                slot = tp_slot_there % 8
                remote(
                    held,
                    cur1.at[slot, :, pl.ds(256 * core, 256)],
                    e_send.at[0],
                    e_recv.at[slot // 4],
                    {"tp": to, "dp": 2 * z + to_core},
                ).start()
            target = cur1.at[0, :, pl.ds(256 * core, 256)]

            @pl.when(to_core == core)
            def _():
                pltpu.make_async_copy(held, target, e_recv.at[0]).start()

            @pl.when(to_core != core)
            def _():
                remote(held, target, e_send_pair, e_recv.at[0], partner).start()
                wait_bytes(held, e_send_pair)

        else:
            final[h] = fresh
            for to, _ in peers:
                remote(
                    final.at[h], final.at[h], e_send.at[1], final_recv, {"tp": to}
                ).start()

    wait_bytes(sq_pair_in, s1_send)
    for half in range(2):
        wait_bytes(pair_in.at[pl.ds(0, 4)], a1_send.at[half])
    wait_bytes(w1.at[0], w1_send)
    wait_bytes(gain1.at[0], g1_send)
    for l in range(2):
        wait_bytes(sq_in.at[l, pl.ds(0, 7)], s2_send.at[l])
        wait_bytes(sums_in.at[l, pl.ds(0, 7)], a2_send.at[l])
        for sem in (ox_send, oy_send):
            wait_bytes(wout.at[l, 0, pl.ds(0, 3), upper], sem.at[l, 0])
            wait_bytes(wout.at[l, pl.ds(0, 3), :, upper], sem.at[l, 1])

        @pl.when(h == d)
        def _():
            wait_bytes(gat_in.at[l, pl.ds(0, 15)], c_send.at[l])

        @pl.when(h != d)
        def _():
            wait_bytes(gat_in.at[l], c_send.at[l])

        wait_bytes(cur.at[pl.ds(0, 15)], e_send.at[l])
    wait_bytes(final.at[pl.ds(0, 15)], final_recv)
    mixed_out[...] = final[...].reshape(256, 256)


def write_out(mixed, state, mixed_out, state_out, sem):
    copies = [pltpu.make_async_copy(mixed, mixed_out, sem.at[8])]
    for n in range(8):
        part = state.at[n // 4, pl.ds(4 * (n % 4), 4)]
        target = state_out.at[n // 4, pl.ds(4 * (n % 4), 4)]
        copies.append(pltpu.make_async_copy(part, target, sem.at[n]))
    for copy in copies:
        copy.start()
    for copy in copies:
        copy.wait()


def per_device(*args):
    any_spec = pl.BlockSpec(memory_space=pl.ANY)
    vmem_spec = pl.BlockSpec(memory_space=pltpu.VMEM)
    dma = pltpu.SemaphoreType.DMA
    shapes = ((256, 256), BF16), ((2, 16, 1, 128, 128), F32)
    held = pl.pallas_call(
        kernel,
        out_shape=tuple(pltpu.VMEM(shape, dtype) for shape, dtype in shapes),
        in_specs=[any_spec] * 10,
        out_specs=(vmem_spec, vmem_spec),
        scratch_shapes=[
            pltpu.VMEM((16, 16, 256), BF16),
            pltpu.VMEM((8, 16, 512), BF16),
            pltpu.VMEM((16, 256), BF16),
            pltpu.VMEM((2, 256), F32),
            pltpu.VMEM((2, 1, 256), F32),
            pltpu.VMEM((256, 512), BF16),
            pltpu.VMEM((2, 256, 512), BF16),
            pltpu.VMEM((2, 128), F32),
            pltpu.VMEM((2, 128), F32),
            pltpu.VMEM((2, 4, 4, 128, 256), BF16),
            pltpu.VMEM((2, 16, 128, 128), F32),
            pltpu.VMEM((16, 16, 512), BF16),
            pltpu.VMEM((8, 16, 512), BF16),
            pltpu.VMEM((2, 8, 16, 512), BF16),
            pltpu.VMEM((2, 8, 16, 512), BF16),
            pltpu.VMEM((2, 1, 128), F32),
            pltpu.VMEM((1, 128), F32),
            pltpu.VMEM((2, 1, 128), F32),
            pltpu.VMEM((2, 8, 1, 128), F32),
            pltpu.VMEM((2, 16, 128), BF16),
            pltpu.VMEM((2, 16, 16, 128), BF16),
            pltpu.VMEM((16, 16, 256), BF16),
            dma((17,)),
            dma,
            dma((2,)),
            dma((2,)),
            dma,
            dma,
            dma,
            dma,
            dma,
            dma,
            dma((2,)),
            dma((2,)),
            dma((2,)),
            dma((2,)),
            dma((2,)),
            dma((2, 4)),
            dma((2, 2)),
            dma((2, 2)),
            dma((2, 2)),
            dma((2, 2)),
            dma((2,)),
            dma((2,)),
            dma,
            dma,
        ],
        compiler_params=pltpu.CompilerParams(collective_id=0, has_side_effects=True),
    )(*args)
    return pl.pallas_call(
        write_out,
        out_shape=tuple(jax.ShapeDtypeStruct(shape, dtype) for shape, dtype in shapes),
        in_specs=[any_spec] * 2,
        out_specs=[any_spec] * 2,
        scratch_shapes=[dma((9,))],
        compiler_params=pltpu.CompilerParams(vmem_limit_bytes=1 << 20),
    )(*held)


def solution(mesh):
    in_specs = (
        P(None, "dp"),
        P(None, "dp"),
        P(None, "dp", "tp"),
        P(None, "dp", "tp"),
        P(None, "dp", "tp"),
        P(None, "dp", "tp"),
        P(None, "tp"),
        P(),
        P(None, "tp", "dp"),
        P(None, "dp", "tp", None, None),
    )
    out_specs = (P(None, "dp"), P(None, "dp", "tp", None, None))
    return jax.shard_map(
        per_device, mesh=mesh, in_specs=in_specs, out_specs=out_specs, check_vma=False
    )
```

```python
import functools

import jax
import jax.numpy as jnp
from jax import lax
from jax.experimental import pallas as pl
from jax.experimental.pallas import tpu as pltpu
from jax.sharding import PartitionSpec as P

D = 4096
DK = 128
EPS = 1e-06
MESH = pl.DeviceIdType.MESH
F32 = jnp.float32
BF16 = jnp.bfloat16

Z_FAR = (4, 3, 5, 2, 6, 1, 7, 0)
TP_GROUPS = (0, 2, 3, 1)


SERVED = ((1, 1), (1, 3), (0, 2), (0, 1), (0, 3), (1, 0), (3, 0))


def gray(v):
    return v + v // 2 - 2 * (v // 3)


def tp_slot(dy, dx):
    return (dx % 2) * 8 + (dx // 2) * 4 + gray(dy)


def kernel(
    tok_in,
    gain_in,
    wq_in,
    wf_in,
    wv_in,
    wg_in,
    floor_in,
    hgain_in,
    wout_in,
    state_in,
    mixed_out,
    state_out,
    cur,
    cur1,
    held,
    gain,
    gain1,
    w0,
    w1,
    floor,
    hgain,
    wout,
    old,
    part,
    pair_in,
    pair,
    sums_in,
    sq,
    sq_pair_in,
    sq_pair,
    sq_in,
    gat,
    gat_in,
    final,
    load_sem,
    tok_sem,
    a1_send,
    a1_recv,
    s1_send,
    s1_recv,
    w1_send,
    w1_recv,
    g1_send,
    g1_recv,
    a2_send,
    a2_recv,
    s2_send,
    s2_recv,
    c_send,
    c_recv,
    ox_send,
    ox_recv,
    oy_send,
    oy_recv,
    e_send,
    e_recv,
    e_send_pair,
    final_recv,
):
    h = lax.axis_index("tp")
    d = lax.axis_index("dp")
    y, x = h // 4, h % 4
    z, core = d // 2, d % 2
    e = (x + core) % 2
    partner = {"dp": 2 * z + 1 - core}

    toks = []
    for dy in range(4):
        for dx in range(4):
            rows = ((y + dy) % 4) * 4 + (x + dx) % 4
            copy = pltpu.make_async_copy(
                tok_in.at[pl.ds(rows * 16, 16), :], cur.at[tp_slot(dy, dx)], tok_sem
            )
            copy.start()
    tok_all = pltpu.make_async_copy(cur, cur, tok_sem)

    loads = {}

    def load(name, src, dst):
        loads[name] = pltpu.make_async_copy(src, dst, load_sem.at[len(loads)])
        loads[name].start()

    weights = (wq_in, wf_in, wv_in, wg_in)
    load("gain", gain_in, gain)
    for n in range(4):
        load(("w", 0, n), weights[n].at[0], w0.at[:, pl.ds(128 * n, 128)])
    def tp_at(dy, dx):
        return ((y + dy) % 4) * 4 + (x + dx) % 4

    antipode = tp_at(2, 2)
    owners = (d, ((d // 4 + 2) % 4) * 4 + (d % 4 + 2) % 4)
    own_copies = jnp.where((owners[0] == h) | (owners[1] == h), 1, 0)

    barrier = pltpu.get_barrier_semaphore()

    def greet(device):
        pl.semaphore_signal(barrier, inc=1, device_id=device, device_id_type=MESH)

    for n in range(1, 8):
        greet({"dp": (d + 2 * n) % 16})
    greet(partner)
    for n in range(1, 16):
        greet({"tp": (h + n) % 16})

    own = pl.multiple_of(8 * e, 8)
    other = pl.multiple_of(8 - 8 * e, 8)
    self_dy = ((2 * z + core) // 4 - y + 4) % 4
    self_dx = ((2 * z + core) % 4 - x + 4) % 4
    self_slot = (self_dx // 2) * 4 + gray(self_dy)
    def remote(src, dst, send, recv, device):
        return pltpu.make_async_remote_copy(
            src_ref=src,
            dst_ref=dst,
            send_sem=send,
            recv_sem=recv,
            device_id=device,
            device_id_type=MESH,
        )

    def wait_bytes(ref, sem):
        pltpu.make_async_copy(ref, ref, sem).wait()

    def project(first, count):
        rows = cur[pl.ds(first, count)].astype(F32).reshape(16 * count, 256)
        normed = (rows * gain[0:1, :]).astype(BF16)
        product = jnp.dot(normed, w0[...], preferred_element_type=F32)
        part[pl.ds(first, count)] = product.astype(BF16).reshape(count, 16, 512)

    def squares(rows):
        ones = jnp.ones((8, rows.shape[1]), BF16)
        square = rows * rows
        high = square.astype(BF16)
        low = (square - high.astype(F32)).astype(BF16)
        dims = (((1,), (1,)), ((), ()))
        total = lax.dot_general(ones, high, dims, preferred_element_type=F32)
        total += lax.dot_general(ones, low, dims, preferred_element_type=F32)
        return total[:1]

    def send_along_z(l, i):
        block = ((y + gray(i % 4)) % 4) * 4 + (x + 2 * (i // 4) + e) % 4
        to_z = block // 2

        @pl.when(to_z != z)
        def _():
            remote(
                pair.at[l, i],
                sums_in.at[l, (z - to_z + 8) % 8],
                a2_send.at[l],
                a2_recv.at[l],
                {"dp": 2 * to_z + core},
            ).start()

    def send_squares_along_z(l):
        for k in range(1, 8):
            remote(
                sq_pair.at[l],
                sq_in.at[l, 8 - k],
                s2_send.at[l],
                s2_recv.at[l],
                {"dp": (d + 2 * k) % 16},
            ).start()

    def along_x(dx):
        return {"tp": y * 4 + (x + dx) % 4}

    def along_y(dy):
        return {"tp": ((y + dy) % 4) * 4 + x}

    upper, lower = pl.ds(0, 64), pl.ds(64, 64)

    def gather_first(l):
        loads["wout", l].wait()
        for n in (2, 1, 3):
            there = tp_slot(0, 4 - n) // 4
            src, dst = wout.at[l, 0, 0, upper], wout.at[l, there, 0, upper]
            remote(src, dst, ox_send.at[l, 0], ox_recv.at[l, 0], along_x(n)).start()
            src, dst = wout.at[l, 0, 0, lower], wout.at[l, 0, gray(4 - n), lower]
            remote(src, dst, oy_send.at[l, 0], oy_recv.at[l, 0], along_y(n)).start()

    def gather_second(l):
        wait_bytes(wout.at[l, 0, pl.ds(0, 3), upper], ox_recv.at[l, 0])
        wait_bytes(wout.at[l, 0, pl.ds(0, 3), lower], oy_recv.at[l, 0])
        for n in (2, 1, 3):
            src, dst = wout.at[l, :, 0, upper], wout.at[l, :, gray(4 - n), upper]
            remote(src, dst, oy_send.at[l, 1], oy_recv.at[l, 1], along_y(n)).start()
            there = tp_slot(0, 4 - n) // 4
            src, dst = wout.at[l, 0, :, lower], wout.at[l, there, :, lower]
            remote(src, dst, ox_send.at[l, 1], ox_recv.at[l, 1], along_x(n)).start()

    for l in range(2):
        if l == 0:
            tok_all.wait()
            loads["gain"].wait()
            for n in range(4):
                loads["w", 0, n].wait()
            project(other, 8)
            load("floor", floor_in, floor)
            load("hgain", hgain_in, hgain)
            load(("state", 0), state_in.at[0, :, 0], old.at[0])
            load(("wout", 0), wout_in.at[0], wout.at[0, 0, 0])
            for n in range(4):
                load(("w", 1, n), weights[n].at[1], w1.at[core, :, pl.ds(128 * n, 128)])
            load(("state", 1), state_in.at[1, :, 0], old.at[1])
            load(("wout", 1), wout_in.at[1], wout.at[1, 0, 0])
            for c in range(2):
                sq[c] = squares(cur[8 * c : 8 * c + 8].astype(F32).reshape(128, 256))
            pl.semaphore_wait(barrier, 23)
            remote(sq.at[1 - e], sq_pair_in, s1_send, s1_recv, partner).start()
            for half in range(2):
                remote(
                    part.at[pl.ds(other + 4 * half, 4)],
                    pair_in.at[pl.ds(4 * half, 4)],
                    a1_send.at[half],
                    a1_recv.at[half],
                    partner,
                ).start()
            gather_first(0)
            project(own, 8)
            wait_bytes(sq_pair_in, s1_recv)
            sq_pair[0] = sq[e] + sq_pair_in[...]
            send_squares_along_z(0)
            for half in range(2):
                wait_bytes(pair_in.at[pl.ds(0, 4)], a1_recv.at[half])
                mine = part[pl.ds(own + 4 * half, 4)].astype(F32)
                theirs = pair_in[4 * half : 4 * half + 4].astype(F32)
                pair[0, 4 * half : 4 * half + 4] = (mine + theirs).astype(BF16)
                for i in range(4):
                    send_along_z(0, 4 * half + i)
        else:
            wait_bytes(w1.at[0], w1_recv)
            wait_bytes(gain1.at[0], g1_recv)
            for half in range(2):
                wait_bytes(cur1.at[pl.ds(0, 4)], e_recv.at[half])
                if half == 1:
                    sq_pair[1] = squares(cur1[...].astype(F32).reshape(128, 512))
                    send_squares_along_z(1)
                rows = cur1[4 * half : 4 * half + 4].astype(F32).reshape(64, 512)
                normed = [(rows[:, 256 * c : 256 * c + 256] * gain1[c]).astype(BF16) for c in range(2)]
                product = jnp.dot(normed[0], w1[0], preferred_element_type=F32)
                product += jnp.dot(normed[1], w1[1], preferred_element_type=F32)
                pair[1, 4 * half : 4 * half + 4] = product.astype(BF16).reshape(4, 16, 512)
                for i in range(4):
                    send_along_z(1, 4 * half + i)
        gather_second(l)

        wait_bytes(sq_in.at[l, pl.ds(0, 7)], s2_recv.at[l])
        row = sq_pair[l]
        for k in range(1, 8):
            row = row + sq_in[l, k]
        lanes = lax.broadcasted_iota(jnp.int32, (16, 128), 1)
        rows = lax.broadcasted_iota(jnp.int32, (16, 128), 0)
        picked = jnp.where(lanes == rows + 16 * self_slot, jnp.broadcast_to(row, (16, 128)), 0.0)
        row_scale = lax.rsqrt(jnp.sum(picked, axis=1, keepdims=True) / D + EPS)
        if l == 0:
            loads["floor"].wait()
            loads["hgain"].wait()
        loads["state", l].wait()
        wait_bytes(sums_in.at[l, pl.ds(0, 7)], a2_recv.at[l])
        total = pair[l, self_slot].astype(F32)
        for k in range(1, 8):
            total = total + sums_in[l, k].astype(F32)
        stored = (row_scale * total).astype(BF16).astype(F32)
        query_pre, forget_pre = stored[:, :128], stored[:, 128:256]
        value, gate_pre = stored[:, 256:384], stored[:, 384:]
        query = jax.nn.silu(query_pre) * DK ** (-0.5)
        low = floor[l : l + 1, :]
        forget = low + (1.0 - low) * jax.nn.sigmoid(forget_pre)
        key_in = (1.0 - low) * jax.nn.sigmoid(-forget_pre)
        scaled = (query * forget).T
        reads = []
        for b in range(16):
            reads.append(jnp.sum(old[l, b] * scaled[:, b : b + 1], axis=0, keepdims=True))
        read = jnp.concatenate(reads, axis=0)
        read = read + jnp.sum(query * key_in, axis=1, keepdims=True) * value
        read = read * lax.rsqrt(jnp.mean(read * read, axis=1, keepdims=True) + EPS)
        gated = read * hgain[l : l + 1, :] * jax.nn.silu(gate_pre)
        gat[l] = gated.astype(BF16)

        places = []
        for b, owner in enumerate(owners):
            slot = tp_slot((y - owner // 4 + 4) % 4, (x - owner % 4 + 4) % 4)
            places.append((owner, gat_in.at[l, 16 * b + slot], c_recv.at[l, slot // 4]))

        def send_read(owner, landing, recv, to):
            remote(gat.at[l], landing, c_send.at[l], recv, {"tp": owner, "dp": to}).start()

        for dz in Z_FAR:
            for other_core in (1, 0):
                to = 2 * ((z + dz) % 8) + (core + other_core) % 2
                for owner, landing, recv in places:
                    if dz or other_core:
                        send_read(owner, landing, recv, to)
                        continue

                    @pl.when(owner != h)
                    def _():
                        send_read(owner, landing, recv, to)

                    @pl.when(owner == h)
                    def _():
                        pltpu.make_async_copy(gat.at[l], landing, recv).start()

        if l == 0:
            for n in range(4):
                loads["w", 1, n].wait()
            remote(w1.at[core], w1.at[core], w1_send, w1_recv, partner).start()
            gain1[core] = gain[1:2, :]
            remote(gain1.at[core], gain1.at[core], g1_send, g1_recv, partner).start()

        forget_t, key_t = forget.T, key_in.T
        for b in range(16):
            kept = old[l, b] * forget_t[:, b : b + 1]
            state_out[l, b, 0] = kept + key_t[:, b : b + 1] * value[b : b + 1, :]

        if l == 0:
            gather_first(1)

        wait_bytes(wout.at[l, pl.ds(0, 3), :, upper], oy_recv.at[l, 1])
        wait_bytes(wout.at[l, pl.ds(0, 3), :, lower], ox_recv.at[l, 1])
        share = jnp.zeros((32, 256), F32)
        for group in TP_GROUPS:
            wait_bytes(gat_in.at[l, pl.ds(0, 8)], c_recv.at[l, group])
            rows = [
                jnp.concatenate([gat_in[l, 16 * b + 4 * group + i] for i in range(4)], axis=1)
                for b in range(2)
            ]
            rows = jnp.concatenate(rows, axis=0)
            columns = wout[l, group].reshape(512, 256)
            share += jnp.dot(rows, columns, preferred_element_type=F32)
        before = [cur[0], cur[tp_slot(2, 2)]] if l == 0 else [held[0], held[1]]
        before = jnp.concatenate(before, axis=0).astype(F32)
        fresh = (before + share).astype(BF16).reshape(2, 16, 256)

        if l == 0:
            held[...] = fresh
            for dy, dx in SERVED:
                for b in range(2):
                    slot = tp_slot((2 * b + 4 - dy) % 4, (2 * b + 4 - dx) % 4) % 8
                    remote(
                        held.at[b],
                        cur1.at[slot, :, pl.ds(256 * core, 256)],
                        e_send.at[0],
                        e_recv.at[slot // 4],
                        {"tp": tp_at(dy, dx), "dp": 2 * z + x % 2},
                    ).start()
            for b in range(2):
                slot = tp_slot(2 * b, 2 * b) % 8
                target = cur1.at[slot, :, pl.ds(256 * core, 256)]

                @pl.when(x % 2 == core)
                def _():
                    pltpu.make_async_copy(held.at[b], target, e_recv.at[slot // 4]).start()

                @pl.when(x % 2 != core)
                def _():
                    remote(held.at[b], target, e_send_pair, e_recv.at[slot // 4], partner).start()

        else:
            final[h] = fresh[0]
            final[antipode] = fresh[1]
            for dy, dx in SERVED:
                for block in (h, antipode):
                    there = final.at[block]
                    remote(there, there, e_send.at[1], final_recv, {"tp": tp_at(dy, dx)}).start()

    wait_bytes(sq_pair_in, s1_send)
    for half in range(2):
        wait_bytes(pair_in.at[pl.ds(0, 4)], a1_send.at[half])
    wait_bytes(w1.at[0], w1_send)
    wait_bytes(gain1.at[0], g1_send)
    for l in range(2):
        wait_bytes(sq_in.at[l, pl.ds(0, 7)], s2_send.at[l])
        wait_bytes(sums_in.at[l, pl.ds(0, 7)], a2_send.at[l])
        for sem in (ox_send, oy_send):
            wait_bytes(wout.at[l, 0, pl.ds(0, 3), upper], sem.at[l, 0])
            wait_bytes(wout.at[l, pl.ds(0, 3), :, upper], sem.at[l, 1])

        @pl.when(own_copies == 1)
        def _():
            wait_bytes(gat_in.at[l, pl.ds(0, 31)], c_send.at[l])

        @pl.when(own_copies == 0)
        def _():
            wait_bytes(gat_in.at[l], c_send.at[l])

        wait_bytes(cur.at[pl.ds(0, 14)], e_send.at[l])

    @pl.when(x % 2 != core)
    def _():
        wait_bytes(held, e_send_pair)

    wait_bytes(final.at[pl.ds(0, 14)], final_recv)
    mixed_out[...] = final[...].reshape(256, 256)


def write_out(mixed, state, mixed_out, state_out, sem):
    copies = [pltpu.make_async_copy(mixed, mixed_out, sem.at[8])]
    for n in range(8):
        part = state.at[n // 4, pl.ds(4 * (n % 4), 4)]
        target = state_out.at[n // 4, pl.ds(4 * (n % 4), 4)]
        copies.append(pltpu.make_async_copy(part, target, sem.at[n]))
    for copy in copies:
        copy.start()
    for copy in copies:
        copy.wait()


def per_device(*args):
    any_spec = pl.BlockSpec(memory_space=pl.ANY)
    vmem_spec = pl.BlockSpec(memory_space=pltpu.VMEM)
    dma = pltpu.SemaphoreType.DMA
    shapes = ((256, 256), BF16), ((2, 16, 1, 128, 128), F32)
    held = pl.pallas_call(
        kernel,
        out_shape=tuple(pltpu.VMEM(shape, dtype) for shape, dtype in shapes),
        in_specs=[any_spec] * 10,
        out_specs=(vmem_spec, vmem_spec),
        scratch_shapes=[
            pltpu.VMEM((16, 16, 256), BF16),
            pltpu.VMEM((8, 16, 512), BF16),
            pltpu.VMEM((2, 16, 256), BF16),
            pltpu.VMEM((2, 256), F32),
            pltpu.VMEM((2, 1, 256), F32),
            pltpu.VMEM((256, 512), BF16),
            pltpu.VMEM((2, 256, 512), BF16),
            pltpu.VMEM((2, 128), F32),
            pltpu.VMEM((2, 128), F32),
            pltpu.VMEM((2, 4, 4, 128, 256), BF16),
            pltpu.VMEM((2, 16, 128, 128), F32),
            pltpu.VMEM((16, 16, 512), BF16),
            pltpu.VMEM((8, 16, 512), BF16),
            pltpu.VMEM((2, 8, 16, 512), BF16),
            pltpu.VMEM((2, 8, 16, 512), BF16),
            pltpu.VMEM((2, 1, 128), F32),
            pltpu.VMEM((1, 128), F32),
            pltpu.VMEM((2, 1, 128), F32),
            pltpu.VMEM((2, 8, 1, 128), F32),
            pltpu.VMEM((2, 16, 128), BF16),
            pltpu.VMEM((2, 32, 16, 128), BF16),
            pltpu.VMEM((16, 16, 256), BF16),
            dma((17,)),
            dma,
            dma((2,)),
            dma((2,)),
            dma,
            dma,
            dma,
            dma,
            dma,
            dma,
            dma((2,)),
            dma((2,)),
            dma((2,)),
            dma((2,)),
            dma((2,)),
            dma((2, 4)),
            dma((2, 2)),
            dma((2, 2)),
            dma((2, 2)),
            dma((2, 2)),
            dma((2,)),
            dma((2,)),
            dma,
            dma,
        ],
        compiler_params=pltpu.CompilerParams(collective_id=0, has_side_effects=True),
    )(*args)
    return pl.pallas_call(
        write_out,
        out_shape=tuple(jax.ShapeDtypeStruct(shape, dtype) for shape, dtype in shapes),
        in_specs=[any_spec] * 2,
        out_specs=[any_spec] * 2,
        scratch_shapes=[dma((9,))],
        compiler_params=pltpu.CompilerParams(vmem_limit_bytes=1 << 20),
    )(*held)


def solution(mesh):
    in_specs = (
        P(None, "dp"),
        P(None, "dp"),
        P(None, "dp", "tp"),
        P(None, "dp", "tp"),
        P(None, "dp", "tp"),
        P(None, "dp", "tp"),
        P(None, "tp"),
        P(),
        P(None, "tp", "dp"),
        P(None, "dp", "tp", None, None),
    )
    out_specs = (P(None, "dp"), P(None, "dp", "tp", None, None))
    return jax.shard_map(
        per_device, mesh=mesh, in_specs=in_specs, out_specs=out_specs, check_vma=False
    )
```
